32 devices in a mesh: grp: 2 (over y), fs: 4 (over z), tp: 4 (over x, core).
Axes of the slice: x: 2, y: 2, z: 4, core: 2. Of those that a mesh axis runs over, the one named last changes fastest.
Arguments:
- tokens: bfloat16 [4096, 2048], P(('grp', 'fs'), 'tp'), parts along dimension 0, may hold values from -6 to 6
- first_gain: bfloat16 [2048], replicated, may hold values from 0.099609375 to 1.8984375
- u_proj: bfloat16 [2048, 1024], P('fs', 'tp'), may hold values from -0.125 to 0.125
- v_proj: bfloat16 [2048, 1024], P('fs', 'tp'), may hold values from -0.125 to 0.125
- group_gain: bfloat16 [8, 128], P('tp'), may hold values from 0.099609375 to 1.8984375
- spatial: bfloat16 [8, 128, 128], P('tp'), may hold values from -0.5 to 0.5
- spatial_bias: bfloat16 [8, 128], P('tp'), may hold values from 0.099609375 to 1.8984375
- mix_proj: bfloat16 [1024, 2048], P('fs', 'tp'), may hold values from -0.1875 to 0.1875
- second_gain: bfloat16 [2048], replicated, may hold values from 0.099609375 to 1.8984375
- up_proj: bfloat16 [2048, 8192], P('fs', 'tp'), may hold values from -0.125 to 0.125
- down_proj: bfloat16 [8192, 2048], P('tp', 'fs'), may hold values from -0.0625 to 0.0625
Outputs:
- layer_out: bfloat16 [4096, 2048], P(('grp', 'fs'), 'tp'), parts along dimension 0
The draws below stay inside these ranges and needn't reach their ends.
There are 2 independent parts, one for each index of `grp`. The reference program is written for one: setup_inputs(seed, part) draws one part's arguments, and reference() takes and returns one part's arrays. A program takes and returns all parts, laid end to end along the dimension named above; an argument that names none is the same for every part. Nothing has to cross between parts.
All inputs are finite; a program needn't handle non-finite values.
Results may differ from the reference program's by a relative error of at most 0.017.
Values may be sent and summed in bfloat16 or wider, within the bound.
A program may use at most 64 MiB of HBM per device.

```python
import jax
import jax.numpy as jnp
from jax import lax

D = 2048
GROUPS = 8
GROUP_DIM = 128
FF = 8192
BLOCK = 128
D_A = 1024
FF_DEV = 2048
TOKENS = 2048


def level_of(key, extent, cuts, least, high):
    level, own = 1.0, jax.random.fold_in(key, 6)
    for dim, shards_of in cuts:
        steps = jnp.exp(jax.random.uniform(jax.random.fold_in(own, dim), (shards_of,), jnp.float32, least / len(cuts), high / len(cuts)))
        level = level * jnp.repeat(steps, extent[dim] // shards_of).reshape([-1 if axis == dim else 1 for axis in range(len(extent))])
    return level


def bell_draw(own_key, extent, width, limit, split=(), kind=jnp.bfloat16):
    values = jax.random.normal(own_key, extent, jnp.float32) * width
    if len(split) > 0:
        values = level_of(own_key, extent, split, -0.22, 0.18) * values
    return jnp.clip(values, min=-limit, max=limit).astype(kind)


def setup_inputs(seed: int = 0, part: int = 0) -> dict:
    arg_keys = jax.random.split(jax.random.key(seed), 12)
    part_keys = jax.random.split(jax.random.fold_in(arg_keys[11], part), 12)
    return {
        "tokens": bell_draw(part_keys[0], (TOKENS, D), 1.0, 6.0, ((0, 4), (1, 4))),
        "first_gain": jnp.clip(1.0 + 0.18 * jax.random.normal(arg_keys[1], (D,), jnp.float32), 0.099609375, 1.8984375).astype(jnp.bfloat16),
        "u_proj": bell_draw(arg_keys[2], (D, D_A), D ** -0.5, 0.125, ((0, 4), (1, 4))),
        "v_proj": bell_draw(arg_keys[3], (D, D_A), D ** -0.5, 0.125, ((0, 4), (1, 4))),
        "group_gain": jnp.clip(1.0 + 0.18 * jax.random.normal(arg_keys[4], (GROUPS, GROUP_DIM), jnp.float32), 0.099609375, 1.8984375).astype(jnp.bfloat16),
        "spatial": bell_draw(arg_keys[5], (GROUPS, BLOCK, BLOCK), BLOCK ** -0.5, 0.5, ((0, 4),)),
        "spatial_bias": jnp.clip(1.0 + 0.18 * jax.random.normal(arg_keys[6], (GROUPS, BLOCK), jnp.float32), 0.099609375, 1.8984375).astype(jnp.bfloat16),
        "mix_proj": bell_draw(arg_keys[7], (D_A, D), D_A ** -0.5, 0.1875, ((0, 4), (1, 4))),
        "second_gain": jnp.clip(1.0 + 0.18 * jax.random.normal(arg_keys[8], (D,), jnp.float32), 0.099609375, 1.8984375).astype(jnp.bfloat16),
        "up_proj": bell_draw(arg_keys[9], (D, FF), D ** -0.5, 0.125, ((0, 4), (1, 4))),
        "down_proj": bell_draw(arg_keys[10], (FF, D), FF ** -0.5, 0.0625, ((0, 4), (1, 4))),
    }


EPS = 1e-06

def rms_scale(values, gain_vec):
    mean_sq = lax.optimization_barrier(jnp.mean(values * values, axis=-1, keepdims=True))
    return values * lax.rsqrt(mean_sq + EPS) * gain_vec.astype(jnp.float32)

def reference(tokens, first_gain, u_proj, v_proj, group_gain, spatial, spatial_bias, mix_proj, second_gain, up_proj, down_proj):
    row_count = tokens.shape[0]
    residual = tokens.astype(jnp.float32)
    normed_rows = rms_scale(residual, first_gain).astype(jnp.bfloat16)
    u_act = jax.nn.gelu(jnp.dot(normed_rows, u_proj, preferred_element_type=jnp.float32)).astype(jnp.bfloat16)
    v_act = jax.nn.gelu(jnp.dot(normed_rows, v_proj, preferred_element_type=jnp.float32))
    v_groups = v_act.reshape(row_count, GROUPS, GROUP_DIM)
    v_normed = rms_scale(v_groups, group_gain).astype(jnp.bfloat16)
    block_view = v_normed.reshape(row_count // BLOCK, BLOCK, GROUPS, GROUP_DIM)
    causal_mask = jnp.tril(jnp.ones((BLOCK, BLOCK), jnp.bool_))
    masked_weights = jnp.where(causal_mask[None], spatial, jnp.zeros_like(spatial))
    mixed_vals = jnp.einsum('gts,nsgd->ntgd', masked_weights.astype(jnp.float32), block_view.astype(jnp.float32))
    mixed_vals = mixed_vals + spatial_bias.astype(jnp.float32).T[None, :, :, None]
    gated_vals = (u_act.astype(jnp.float32) * mixed_vals.reshape(row_count, GROUPS * GROUP_DIM)).astype(jnp.bfloat16)
    mix_vals = jnp.dot(gated_vals, mix_proj, preferred_element_type=jnp.float32)
    mid_stream = (residual + mix_vals).astype(jnp.bfloat16)
    normed_two = rms_scale(mid_stream.astype(jnp.float32), second_gain).astype(jnp.bfloat16)
    pre_act = jnp.dot(normed_two, up_proj, preferred_element_type=jnp.float32)
    hidden_act = jnp.square(jax.nn.relu(pre_act)).astype(jnp.bfloat16)
    down_sum = jnp.zeros((row_count, D), jnp.float32)
    for block_idx in range(FF // FF_DEV):
        first_row = block_idx * FF_DEV
        partial_prod = jnp.dot(hidden_act[:, first_row:first_row + FF_DEV], down_proj[first_row:first_row + FF_DEV], preferred_element_type=jnp.float32)
        rounded_part = lax.optimization_barrier(partial_prod.astype(jnp.bfloat16))
        down_sum = down_sum + rounded_part.astype(jnp.float32)
    return (mid_stream.astype(jnp.float32) + down_sum).astype(jnp.bfloat16)
```

```python
import functools

import jax
import jax.numpy as jnp
from jax import lax
from jax.experimental import pallas as pl
from jax.experimental.pallas import tpu as pltpu
from jax.sharding import PartitionSpec as P

EPS = 1e-06


def rms_scale(values, gain_vec):
    mean_sq = jnp.mean(values * values, axis=-1, keepdims=True)
    return values * lax.rsqrt(mean_sq + EPS) * gain_vec.astype(jnp.float32)


def per_device(
    tokens,
    first_gain,
    u_proj,
    v_proj,
    group_gain,
    spatial,
    spatial_bias,
    mix_proj,
    second_gain,
    up_proj,
    down_proj,
):
    whole_rows = lax.all_gather(tokens, "tp", axis=1, tiled=True)
    row_count = whole_rows.shape[0]
    normed_rows = rms_scale(whole_rows.astype(jnp.float32), first_gain).astype(jnp.bfloat16)
    local_width = u_proj.shape[1]
    column_part = normed_rows
    u_pre = jnp.dot(
        column_part,
        lax.all_gather(u_proj, "fs", axis=0, tiled=True),
        preferred_element_type=jnp.float32,
    )
    v_pre = jnp.dot(
        column_part,
        lax.all_gather(v_proj, "fs", axis=0, tiled=True),
        preferred_element_type=jnp.float32,
    )
    u_act = jax.nn.gelu(u_pre).astype(jnp.bfloat16)
    local_groups = group_gain.shape[0]
    group_width = group_gain.shape[1]
    v_groups = jax.nn.gelu(v_pre).reshape(row_count, local_groups, group_width)
    v_normed = rms_scale(v_groups, group_gain).astype(jnp.bfloat16)
    block_len = spatial.shape[1]
    block_view = v_normed.reshape(row_count // block_len, block_len, local_groups, group_width)
    causal_mask = jnp.tril(jnp.ones((block_len, block_len), jnp.bool_))
    masked_weights = jnp.where(causal_mask[None], spatial, jnp.zeros_like(spatial))
    mixed_vals = jnp.einsum(
        "gts,nsgd->ntgd", masked_weights, block_view, preferred_element_type=jnp.float32
    )
    mixed_vals = mixed_vals + spatial_bias.astype(jnp.float32).T[None, :, :, None]
    gated_vals = (u_act.astype(jnp.float32) * mixed_vals.reshape(row_count, local_width)).astype(
        jnp.bfloat16
    )
    gated_whole = lax.all_gather(gated_vals, "tp", axis=1, tiled=True)
    column_part = gated_whole
    mix_vals = jnp.dot(
        column_part,
        lax.all_gather(mix_proj, "fs", axis=0, tiled=True),
        preferred_element_type=jnp.float32,
    )
    mid_stream = (tokens.astype(jnp.float32) + mix_vals).astype(jnp.bfloat16)
    mid_whole = lax.all_gather(mid_stream, "tp", axis=1, tiled=True)
    normed_two = rms_scale(mid_whole.astype(jnp.float32), second_gain).astype(jnp.bfloat16)
    column_part = normed_two
    pre_act = jnp.dot(
        column_part,
        lax.all_gather(up_proj, "fs", axis=0, tiled=True),
        preferred_element_type=jnp.float32,
    )
    hidden_act = jnp.square(jax.nn.relu(pre_act)).astype(jnp.bfloat16)
    down_terms = jnp.dot(
        hidden_act,
        lax.all_gather(down_proj, "fs", axis=1, tiled=True),
        preferred_element_type=jnp.float32,
    )
    down_sum = lax.psum_scatter(
        down_terms.astype(jnp.bfloat16), "tp", scatter_dimension=1, tiled=True
    ).astype(jnp.float32)
    return (mid_stream.astype(jnp.float32) + down_sum).astype(jnp.bfloat16)


def remote(src, dst, send, recv, where):
    return pltpu.make_async_remote_copy(
        src_ref=src,
        dst_ref=dst,
        send_sem=send,
        recv_sem=recv,
        device_id=where,
        device_id_type=pl.DeviceIdType.MESH,
    )


def fused_kernel(
    row_step,
    tok, gain1, u_w, v_w, ggain, spat, bias, mix_w, gain2, up_w, down_w,
    out,
    xg, uvg, mg, upg, dng, norm, gat, mid, hid, c_out, c_in, z_out, z_in, z_part, x_in, x_out, x_part,
    acc,
    h_send, z_send, z_recv, y_send, y_recv, l_sem, a_send, a_recv, c_send, c_recv, r_send,
    r_recv, s_send, s_recv, p_send, p_recv, o_send, o_recv,
):
    y, z, t = lax.axis_index("grp"), lax.axis_index("fs"), lax.axis_index("tp")
    q, c, x = lax.rem(z, 2), lax.rem(t, 2), t // 2
    z_pair = z + 1 - 2 * q
    t_core, t_chip = t + 1 - 2 * c, lax.rem(t + 2, 4)
    to_y, to_z = (1 - y, z, t), (y, z_pair, t)
    to_c, to_x = (y, z, t_core), (y, z, t_chip)
    across, facing, pair = others = (lax.rem(z + 2, 4), 3 - z, z_pair)
    rows, width = tok.shape
    step, z_count = row_step, dng.shape[0]
    f32, bf16 = jnp.float32, jnp.bfloat16

    barrier = pltpu.get_barrier_semaphore()
    for where in (to_y, to_c, to_x) + tuple((y, o, t) for o in others):
        pl.semaphore_signal(
            barrier, inc=1, device_id=where, device_id_type=pl.DeviceIdType.MESH
        )
    pl.semaphore_wait(barrier, 6)

    gw, da = ggain.shape[1], u_w.shape[1]
    ur, mr, pr = u_w.shape[0], mix_w.shape[0], up_w.shape[0]
    ff, inner_ff = up_w.shape[1], hid.shape[1]
    share = (ff - inner_ff, inner_ff)

    def half(size, which):
        return pl.ds(pl.multiple_of(which * size, size), size)

    cuts = dng.shape[1]
    cut = width // cuts
    parts = (1, 1, 1, 2, cuts)

    def slab(size, which, start=0):
        if which is None:
            return pl.ds(start, size)
        return pl.ds(pl.multiple_of(start + which * (size // 2), 16), size // 2)

    def take(w, role, which, k=0):
        shard = (u_w, v_w, mix_w, up_w, down_w)[w]
        size, start = share[role], role * share[0]
        if w == 4:
            return shard.at[slab(size, which, start), pl.ds(k * cut, cut)]
        tall = shard.shape[0]
        cols = slice(None) if w < 3 else pl.ds(start, size)
        if which is None:
            return shard.at[:, cols]
        return shard.at[half(tall // 2 // parts[w], parts[w] * which + k), cols]

    def put(w, role, source, which, k=0):
        n, size = parts[w], share[role]
        if w == 4:
            return dng.at[source, k, slab(size, which), :]
        whole, tall = ((uvg, ur), (uvg, ur), (mg, mr), (upg, pr))[w]
        cols = pl.ds(w * da, da) if w < 2 else slice(None) if w < 3 else pl.ds(0, size)
        if which is None:
            return whole.at[half(tall, source), cols]
        return whole.at[half(tall // 2 // n, n * (2 * source + which) + k), cols]

    def z_piece(w, role, dest, k):
        return remote(
            take(w, role, y, k), put(w, role, z, y, k), z_send.at[w, dest, k],
            z_recv.at[w, z, k], (y, dest, t),
        )

    def z_start(w, role, dest, ks=None):
        for k in range(parts[w]) if ks is None else ks:
            z_piece(w, role, dest, k).start()

    def y_piece(w, role, source, k):
        ref = put(w, role, source, y, k)
        return remote(ref, ref, y_send.at[w, source, k], y_recv.at[w, source, k], to_y)

    def y_arrived(w, role, source, k):
        ref = put(w, role, source, 1 - y, k)
        remote(
            ref, ref, y_send.at[w, source, k], y_recv.at[w, source, k], to_y
        ).wait_recv()

    def y_all(w, role):
        for o in others:
            for k in range(parts[w]):
                y_arrived(w, role, o, k)

    def relay(w, role, source, k):
        ref = put(w, role, source, y, k)
        remote(
            ref, ref, z_send.at[w, source, k], z_recv.at[w, source, k], (y, source, t)
        ).wait_recv()
        y_piece(w, role, source, k).start()

    def relays(w, role, source, ks=None):
        for k in range(parts[w]) if ks is None else ks:
            relay(w, role, source, k)

    def hop(w, source, way, own=False):
        ref = put(w, 0, source, y)
        return remote(
            take(w, 0, y) if own else ref, ref, h_send.at[w, source, way],
            z_recv.at[w, source, 0], (y, z + 1 - 2 * way, t),
        )

    last = z_count - 1
    goes_on = (z < last, z > 0)

    def chain(w, distance):
        for way in range(2):
            source = z - distance if way == 0 else z + distance

            @pl.when(source >= 0 if way == 0 else source <= last)
            def _():
                hop(w, source, way).wait_recv()

                @pl.when(goes_on[way])
                def _():
                    hop(w, source, way).start()

                y_piece(w, 0, source, 0).start()

    def own_copies(w, role):
        return [
            pltpu.make_async_copy(
                take(w, role, None, k), put(w, role, z, None, k), l_sem.at[w + k]
            )
            for k in range(cuts if w == 4 else 1)
        ]

    def gather_copy(a, h, n):
        p, s, where = (
            (q, t, to_z), (q, t, to_x), (q, t, to_c), (1 - q, t, to_x), (1 - q, t, to_c),
            (q, t_chip, to_c), (1 - q, t_chip, to_c),
        )[n]
        ref = piece(a, h, p, s)
        return remote(ref, ref, a_send.at[a, h, n], a_recv.at[a, h, n], where)

    def gather_arrived(a, h, n):
        p, s, where = (
            (1 - q, t, to_z), (q, t_chip, to_x), (q, t_core, to_c), (1 - q, t_chip, to_x),
            (1 - q, t_core, to_c), (q, 3 - t, to_c), (1 - q, 3 - t, to_c),
        )[n]
        ref = piece(a, h, p, s)
        return remote(ref, ref, a_send.at[a, h, n], a_recv.at[a, h, n], where)

    def piece(a, h, p, s):
        if a == 0:
            return xg.at[s, pl.ds(h * step, step), :]
        return gat.at[s, h] if a == 1 else mid.at[p, s, h]

    def gather_start(a, h):
        for n in (1, 2, 0)[: 3 if a == 2 else 2]:
            gather_copy(a, h, n).start()

    def gather_pair(a, h):
        gather_arrived(a, h, 0).wait_recv()
        gather_copy(a, h, 3).start()
        gather_copy(a, h, 4).start()

    def gather_rest(a, h):
        gather_arrived(a, h, 1).wait_recv()
        gather_copy(a, h, 5).start()
        if a == 2:
            gather_arrived(a, h, 3).wait_recv()
            gather_copy(a, h, 6).start()
        for n in (2, 4, 5, 6) if a == 2 else (2, 5):
            gather_arrived(a, h, n).wait_recv()

    chunks = rows // step
    inner = jnp.logical_and(z > 0, z < last)

    own_tok = pltpu.make_async_copy(tok, xg.at[t], l_sem.at[4 + cuts])
    own_tok.start()
    for w in range(3):
        for way in range(2):
            @pl.when(goes_on[way])
            def _():
                hop(w, z, way, True).start()
    own_tok.wait()
    for h in range(chunks):
        gather_start(0, h)
    def scaled(pieces, gain):
        total = pieces[0].shape[0]
        sums = jnp.zeros((total, 1), f32)
        for piece in pieces:
            sums += jnp.sum(piece * piece, axis=-1, keepdims=True)
        count = sum(piece.shape[1] for piece in pieces)
        scale = lax.rsqrt(sums / count + EPS)
        at = 0
        res = []
        for piece in pieces:
            wide = piece.shape[1]
            res.append((piece * scale * gain[:, at : at + wide]).astype(bf16))
            at += wide
        return jnp.concatenate(res, axis=1)

    small = 64
    per_part = step // small
    gain_one = gain1[...].astype(f32).reshape(1, -1)
    gain_two = gain2[...].astype(f32).reshape(1, -1)

    def norm_one(h):
        def loop(i, carry):
            here = pl.ds(pl.multiple_of(h * step + i * small, small), small)
            norm[here, :] = scaled([xg[s, here, :].astype(f32) for s in range(4)], gain_one)
            return carry

        lax.fori_loop(0, per_part, loop, 0)

    blk = spat.shape[1]
    lower = lax.broadcasted_iota(jnp.int32, (blk, blk), 0) >= lax.broadcasted_iota(
        jnp.int32, (blk, blk), 1
    )
    eye = lax.broadcasted_iota(jnp.int32, (blk, blk), 0) == lax.broadcasted_iota(
        jnp.int32, (blk, blk), 1
    )
    mixers, shifts, gains = [], [], []
    for g in range(da // gw):
        mixers.append(jnp.where(lower, spat[g].astype(f32), 0.0).astype(bf16))
        column = jnp.where(eye, bias[g : g + 1, :].astype(f32), 0.0)
        shifts.append(jnp.sum(column, axis=1, keepdims=True))
        gains.append(ggain[g : g + 1, :].astype(f32))

    def mix_rows(h):
        both = jnp.dot(norm[pl.ds(h * step, step), :], uvg[...], preferred_element_type=f32)
        both = jax.nn.gelu(both)
        u_act = both[:, :da].astype(bf16).astype(f32)
        for g in range(da // gw):
            cols = slice(g * gw, (g + 1) * gw)
            v_act = both[:, da + g * gw : da + (g + 1) * gw]
            v_n = (
                v_act
                * lax.rsqrt(jnp.mean(v_act * v_act, axis=-1, keepdims=True) + EPS)
                * gains[g]
            ).astype(bf16)
            for b in range(step // blk):
                part = slice(b * blk, (b + 1) * blk)
                mixed = jnp.dot(mixers[g], v_n[part], preferred_element_type=f32) + shifts[g]
                gat[t, h, part, cols] = (u_act[part, cols] * mixed).astype(bf16)

    def middle_rows(h):
        left = jnp.concatenate([gat[k, h] for k in range(4)], axis=1)
        value = jnp.dot(left, mg[...], preferred_element_type=f32)
        value += tok[pl.ds(h * step, step), :].astype(f32)
        mid[q, t, h] = value.astype(bf16)

    def norm_two(h):
        def loop(i, carry):
            p, r = i // per_part, pl.multiple_of(lax.rem(i, per_part) * small, small)
            pieces = [mid[p, k, h, pl.ds(r, small), :].astype(f32) for k in range(4)]
            at = pl.multiple_of(h * 2 * step + i * small, small)
            norm[pl.ds(at, small), :] = scaled(pieces, gain_two)
            return carry

        lax.fori_loop(0, 2 * per_part, loop, 0)

    def up_rows(h, role):
        size = share[role]

        def loop(i, carry):
            here = pl.ds(pl.multiple_of((2 * h + i) * step, step), step)
            pre = jnp.dot(norm[here, :], upg[:, :size], preferred_element_type=f32)
            hid[here, :size] = jnp.square(jax.nn.relu(pre)).astype(bf16)
            return carry

        lax.fori_loop(0, 2, loop, 0)

    def part(quarter, k, b, role):
        start, size = pl.multiple_of(b * step, step), share[role]
        return jnp.dot(
            hid[pl.ds(start, step), :size], dng[quarter, k, :size],
            preferred_element_type=f32,
        )

    def core_copy(n, k):
        return remote(
            c_out.at[n, k], c_in.at[n, k], c_send.at[n, k], c_recv.at[n, k], to_c
        )

    wide_n, slim_n = c, 1 - c
    own_wide = x == c

    def wide_x(k):
        return remote(c_in.at[wide_n, k], x_in.at[k], s_send.at[k], s_recv.at[k], to_x)

    def wide_z(k):
        return remote(z_out.at[k], z_in.at[k], r_send.at[k], r_recv.at[k], to_z)

    def slim_z(k):
        return remote(
            c_in.at[slim_n, k, 1 - q], z_part.at[k], p_send.at[k], p_recv.at[k], to_z
        )

    def slim_x(k):
        return remote(x_out.at[k], x_part.at[k], o_send.at[k], o_recv.at[k], to_x)

    def down(quarter, k, role):
        n = quarter // 2
        mine = lax.rem(quarter, 2) == c

        @pl.when(jnp.logical_not(mine))
        def _():
            def loop(b, carry):
                c_out[n, k, lax.rem(b, 2), b // 2] = part(quarter, k, b, role).astype(bf16)
                return carry

            lax.fori_loop(0, 2 * chunks, loop, 0)
            core_copy(n, k).start()

        @pl.when(mine)
        def _():
            def loop(b, carry):
                acc[b] = part(quarter, k, b, role)
                return carry

            lax.fori_loop(0, 2 * chunks, loop, 0)
            core_copy(n, k).wait_recv()

            def add(b, carry):
                p, h = lax.rem(b, 2), b // 2
                value = acc[b] + c_in[n, k, p, h].astype(f32)
                c_in[n, k, p, h] = value.astype(bf16)
                return carry

            lax.fori_loop(0, 2 * chunks, add, 0)

            @pl.when((n == wide_n) & jnp.logical_not(own_wide))
            def _():
                wide_x(k).start()

            @pl.when(n == slim_n)
            def _():
                slim_z(k).start()

    def meet(role):
        @pl.when(own_wide)
        def _():
            for k in every:
                wide_x(k).wait_recv()
                for h in range(chunks):
                    value = c_in[wide_n, k, 1 - q, h].astype(f32)
                    value += x_in[k, 1 - q, h].astype(f32)
                    z_out[k, h] = value.astype(bf16)
                wide_z(k).start()

    every = range(cuts)
    early, late = every[: cuts // 2], every[cuts // 2 :]

    def mixer():
        for w in range(2):
            for copy in own_copies(w, 0):
                copy.wait()
            y_all(w, 0)
        for h in range(chunks):
            mix_rows(h)
            gather_start(1, h)

    def middle():
        for copy in own_copies(2, 0):
            copy.wait()
        y_all(2, 0)
        for h in range(chunks):
            gather_rest(1, h)
            middle_rows(h)
            gather_start(2, h)

    def widen(role):
        for copy in own_copies(3, role):
            copy.wait()
        y_all(3, role)
        for h in range(chunks):
            up_rows(h, role)
        for copy in own_copies(4, role):
            copy.wait()

    def downs(role, source, ks=None):
        for k in every if ks is None else ks:
            y_arrived(4, role, source, k)
            down(source, k, role)

    def start(role):
        for w in range(5):
            for copy in own_copies(w, role):
                copy.start()

    @pl.when(jnp.logical_not(inner))
    def _():
        start(0)
        z_start(3, 1, pair)
        z_start(3, 1, across)
        z_start(4, 1, across, early)
        for w in range(3):
            chain(w, 1)
        for h in range(chunks):
            gather_rest(0, h)
            norm_one(h)
        for d in range(2, z_count):
            for w in range(3):
                chain(w, d)
        mixer()
        middle()
        z_start(4, 1, across, late[:1])
        z_start(3, 0, facing)
        z_start(4, 1, pair)
        z_start(4, 1, across, late[1:])
        z_start(4, 0, facing)
        relays(3, 0, pair)
        gather_pair(2, 0)
        gather_pair(2, 1)
        gather_rest(2, 0)
        norm_two(0)
        relay(3, 0, facing, 0)
        gather_rest(2, 1)
        norm_two(1)
        relay(3, 0, facing, 1)
        relays(3, 0, across)
        widen(0)
        for k in every:
            down(z, k, 0)
        relays(4, 0, pair, early[:1])
        relays(4, 0, facing)
        relays(4, 0, across, early)
        downs(0, facing)
        relays(4, 0, across, late)
        downs(0, across)
        relays(4, 0, pair, every[1:])
        downs(0, pair)
        meet(0)

    @pl.when(inner)
    def _():
        start(1)
        for w in range(3):
            chain(w, 1)
        z_start(3, 1, facing)
        z_start(4, 1, facing, early[:1])
        z_start(3, 0, across)
        z_start(4, 0, across)
        z_start(4, 1, facing, every[1:])
        for h in range(chunks):
            gather_rest(0, h)
            norm_one(h)
        for w in range(3):
            chain(w, 2)
        z_start(3, 0, pair)
        for w in range(3):
            chain(w, 3)
        relays(3, 1, pair)
        mixer()
        relays(3, 1, across)
        middle()
        z_start(4, 0, pair)
        relay(3, 1, facing, 0)
        gather_pair(2, 0)
        relay(3, 1, facing, 1)
        gather_pair(2, 1)
        relays(4, 1, across, early)
        gather_rest(2, 0)
        norm_two(0)
        gather_rest(2, 1)
        norm_two(1)
        widen(1)
        relays(4, 1, across, late)
        for k in every:
            down(z, k, 1)
        relays(4, 1, pair)
        downs(1, across)
        downs(1, pair)
        relays(4, 1, facing)
        meet(1)
        downs(1, facing)

    def result(value, k, h):
        cols = slice(k * cut, (k + 1) * cut)
        value += mid[q, t, h, :, cols].astype(f32)
        out[pl.ds(h * step, step), cols] = value.astype(bf16)

    @pl.when(own_wide)
    def _():
        for k in every:
            slim_z(k).wait_recv()
            for h in range(chunks):
                value = c_in[slim_n, k, q, h].astype(f32) + z_part[k, h].astype(f32)
                x_out[k, h] = value.astype(bf16)
            slim_x(k).start()
        for k in every:
            wide_z(k).wait_recv()
            for h in range(chunks):
                value = c_in[wide_n, k, q, h].astype(f32) + x_in[k, q, h].astype(f32)
                result(value + z_in[k, h].astype(f32), k, h)
        for k in every:
            wide_z(k).wait_send()
            slim_x(k).wait_send()

    @pl.when(jnp.logical_not(own_wide))
    def _():
        for k in every:
            slim_z(k).wait_recv()
            slim_x(k).wait_recv()
            for h in range(chunks):
                value = c_in[slim_n, k, q, h].astype(f32) + z_part[k, h].astype(f32)
                result(value + x_part[k, h].astype(f32), k, h)
        for k in every:
            wide_x(k).wait_send()

    def drain(role):
        for w in range(5):
            for o, other in ((across, 1 - role), (facing, role), (pair, 1 - role)):
                for k in range(parts[w]):
                    if w > 2:
                        z_piece(w, other, o, k).wait_send()
                    y_piece(w, role, o, k).wait_send()

    @pl.when(jnp.logical_not(inner))
    def _():
        drain(0)

    @pl.when(inner)
    def _():
        drain(1)

    for w in range(3):
        for source in range(z_count):
            for way in range(2):
                came = source <= z if way == 0 else source >= z

                @pl.when(came & goes_on[way])
                def _():
                    hop(w, source, way).wait_send()

    for h in range(chunks):
        for a in range(3):
            for n in range(7) if a == 2 else (1, 2, 5):
                gather_copy(a, h, n).wait_send()
    for k in every:
        for n in range(2):
            core_copy(n, k).wait_send()
        slim_z(k).wait_send()


def fused(tokens, first_gain, u_proj, v_proj, group_gain, spatial, spatial_bias, mix_proj,
          second_gain, up_proj, down_proj):
    rows, width = tokens.shape
    both, wide, da = 2 * rows, second_gain.shape[0], u_proj.shape[1]
    vmem, bf16, dma = pltpu.VMEM, jnp.bfloat16, pltpu.SemaphoreType.DMA
    spec = pl.BlockSpec(memory_space=pltpu.VMEM)
    ff = up_proj.shape[1] // 16 * 9
    step = 256
    chunks = rows // step
    cuts = 4
    cut = width // cuts
    return pl.pallas_call(
        functools.partial(fused_kernel, step),
        out_shape=jax.ShapeDtypeStruct(tokens.shape, tokens.dtype),
        in_specs=[spec] * 11,
        out_specs=spec,
        scratch_shapes=[
            vmem((4, rows, width), bf16),
            vmem((wide, 2 * da), bf16),
            vmem((4 * mix_proj.shape[0], width), bf16),
            vmem((wide, ff), bf16),
            vmem((4, cuts, ff, cut), bf16),
            vmem((both, wide), bf16),
            vmem((4, chunks, step, da), bf16),
            vmem((2, 4, chunks, step, width), bf16),
            vmem((both, ff), bf16),
            vmem((2, cuts, 2, chunks, step, cut), bf16),
            vmem((2, cuts, 2, chunks, step, cut), bf16),
            vmem((cuts, chunks, step, cut), bf16),
            vmem((cuts, chunks, step, cut), bf16),
            vmem((cuts, chunks, step, cut), bf16),
            vmem((cuts, 2, chunks, step, cut), bf16),
            vmem((cuts, chunks, step, cut), bf16),
            vmem((cuts, chunks, step, cut), bf16),
            vmem((2 * chunks, step, cut), jnp.float32),
            dma((3, 4, 2)),
            dma((5, 4, 4)), dma((5, 4, 4)), dma((5, 4, 4)), dma((5, 4, 4)), dma((5 + cuts,)),
            dma((3, chunks, 7)), dma((3, chunks, 7)),
            dma((2, cuts)), dma((2, cuts)), dma((cuts,)), dma((cuts,)),
            dma((cuts,)), dma((cuts,)), dma((cuts,)), dma((cuts,)), dma((cuts,)),
            dma((cuts,)),
        ],
        compiler_params=pltpu.CompilerParams(
            collective_id=0, has_side_effects=True, vmem_limit_bytes=64 * 1024 * 1000
        ),
    )(
        tokens, first_gain, u_proj, v_proj, group_gain, spatial, spatial_bias, mix_proj,
        second_gain, up_proj, down_proj,
    )


def layer_part(axes, *args):
    tokens, group_gain, spatial = args[0], args[4], args[5]
    fits = (
        axes["grp"] == 2
        and axes["fs"] == 4
        and axes["tp"] == 4
        and group_gain.shape[0] == 2
        and group_gain.shape[1] % 128 == 0
        and tokens.shape[0] % 256 == 0
        and tokens.shape[1] % 256 == 0
        and tokens.shape[1] == args[10].shape[1]
        and 256 % spatial.shape[1] == 0
        and args[9].shape[1] % 2048 == 0
    )
    return fused(*args) if fits else per_device(*args)


def solution(mesh):
    return jax.shard_map(
        functools.partial(layer_part, dict(mesh.shape)),
        mesh=mesh,
        in_specs=(
            P(("grp", "fs"), "tp"),
            P(),
            P("fs", "tp"),
            P("fs", "tp"),
            P("tp", None),
            P("tp", None, None),
            P("tp", None),
            P("fs", "tp"),
            P(),
            P("fs", "tp"),
            P("tp", "fs"),
        ),
        out_specs=P(("grp", "fs"), "tp"),
        check_vma=False,
    )
```

```python
import functools

import jax
import jax.numpy as jnp
from jax import lax
from jax.experimental import pallas as pl
from jax.experimental.pallas import tpu as pltpu
from jax.sharding import PartitionSpec as P

EPS = 1e-06


def rms_scale(values, gain_vec):
    mean_sq = jnp.mean(values * values, axis=-1, keepdims=True)
    return values * lax.rsqrt(mean_sq + EPS) * gain_vec.astype(jnp.float32)


def per_device(
    tokens,
    first_gain,
    u_proj,
    v_proj,
    group_gain,
    spatial,
    spatial_bias,
    mix_proj,
    second_gain,
    up_proj,
    down_proj,
):
    whole_rows = lax.all_gather(tokens, "tp", axis=1, tiled=True)
    row_count = whole_rows.shape[0]
    normed_rows = rms_scale(whole_rows.astype(jnp.float32), first_gain).astype(jnp.bfloat16)
    local_width = u_proj.shape[1]
    column_part = normed_rows
    u_pre = jnp.dot(
        column_part,
        lax.all_gather(u_proj, "fs", axis=0, tiled=True),
        preferred_element_type=jnp.float32,
    )
    v_pre = jnp.dot(
        column_part,
        lax.all_gather(v_proj, "fs", axis=0, tiled=True),
        preferred_element_type=jnp.float32,
    )
    u_act = jax.nn.gelu(u_pre).astype(jnp.bfloat16)
    local_groups = group_gain.shape[0]
    group_width = group_gain.shape[1]
    v_groups = jax.nn.gelu(v_pre).reshape(row_count, local_groups, group_width)
    v_normed = rms_scale(v_groups, group_gain).astype(jnp.bfloat16)
    block_len = spatial.shape[1]
    block_view = v_normed.reshape(row_count // block_len, block_len, local_groups, group_width)
    causal_mask = jnp.tril(jnp.ones((block_len, block_len), jnp.bool_))
    masked_weights = jnp.where(causal_mask[None], spatial, jnp.zeros_like(spatial))
    mixed_vals = jnp.einsum(
        "gts,nsgd->ntgd", masked_weights, block_view, preferred_element_type=jnp.float32
    )
    mixed_vals = mixed_vals + spatial_bias.astype(jnp.float32).T[None, :, :, None]
    gated_vals = (u_act.astype(jnp.float32) * mixed_vals.reshape(row_count, local_width)).astype(
        jnp.bfloat16
    )
    gated_whole = lax.all_gather(gated_vals, "tp", axis=1, tiled=True)
    column_part = gated_whole
    mix_vals = jnp.dot(
        column_part,
        lax.all_gather(mix_proj, "fs", axis=0, tiled=True),
        preferred_element_type=jnp.float32,
    )
    mid_stream = (tokens.astype(jnp.float32) + mix_vals).astype(jnp.bfloat16)
    mid_whole = lax.all_gather(mid_stream, "tp", axis=1, tiled=True)
    normed_two = rms_scale(mid_whole.astype(jnp.float32), second_gain).astype(jnp.bfloat16)
    column_part = normed_two
    pre_act = jnp.dot(
        column_part,
        lax.all_gather(up_proj, "fs", axis=0, tiled=True),
        preferred_element_type=jnp.float32,
    )
    hidden_act = jnp.square(jax.nn.relu(pre_act)).astype(jnp.bfloat16)
    down_terms = jnp.dot(
        hidden_act,
        lax.all_gather(down_proj, "fs", axis=1, tiled=True),
        preferred_element_type=jnp.float32,
    )
    down_sum = lax.psum_scatter(
        down_terms.astype(jnp.bfloat16), "tp", scatter_dimension=1, tiled=True
    ).astype(jnp.float32)
    return (mid_stream.astype(jnp.float32) + down_sum).astype(jnp.bfloat16)


def remote(src, dst, send, recv, where):
    return pltpu.make_async_remote_copy(
        src_ref=src,
        dst_ref=dst,
        send_sem=send,
        recv_sem=recv,
        device_id=where,
        device_id_type=pl.DeviceIdType.MESH,
    )


def fused_kernel(
    row_step, piece_cuts,
    tok, gain1, u_w, v_w, ggain, spat, bias, mix_w, gain2, up_w, down_w,
    out,
    xg, uvg, mg, upg, dng, norm, gat, mid, hid, c_out, c_in, z_out, z_in, z_part, x_in, x_out, x_part,
    acc,
    h_send, z_send, z_recv, y_send, y_recv, l_sem, a_send, a_recv, c_send, c_recv, r_send,
    r_recv, s_send, s_recv, p_send, p_recv, o_send, o_recv,
):
    y, z, t = lax.axis_index("grp"), lax.axis_index("fs"), lax.axis_index("tp")
    q, c, x = lax.rem(z, 2), lax.rem(t, 2), t // 2
    z_pair = z + 1 - 2 * q
    t_core, t_chip = t + 1 - 2 * c, lax.rem(t + 2, 4)
    to_y, to_z = (1 - y, z, t), (y, z_pair, t)
    to_c, to_x = (y, z, t_core), (y, z, t_chip)
    across, facing, pair = others = (lax.rem(z + 2, 4), 3 - z, z_pair)
    rows, width = tok.shape
    step, z_count = row_step, dng.shape[0]
    f32, bf16 = jnp.float32, jnp.bfloat16

    barrier = pltpu.get_barrier_semaphore()
    for where in (to_y, to_c, to_x) + tuple((y, o, t) for o in others):
        pl.semaphore_signal(
            barrier, inc=1, device_id=where, device_id_type=pl.DeviceIdType.MESH
        )
    pl.semaphore_wait(barrier, 6)

    gw, da = ggain.shape[1], u_w.shape[1]
    ur, mr, pr = u_w.shape[0], mix_w.shape[0], up_w.shape[0]
    ff, inner_ff = up_w.shape[1], hid.shape[1]
    share = (ff - inner_ff, inner_ff)

    def half(size, which):
        return pl.ds(pl.multiple_of(which * size, size), size)

    cuts, cut = piece_cuts, width // piece_cuts
    cols, col = c_out.shape[1], c_out.shape[3]
    parts = (1, 1, 1, 2, cuts)

    def lane(w, k):
        return sum(parts[:w]) + k

    def slab(size, which, start=0):
        if which is None:
            return pl.ds(start, size)
        return pl.ds(pl.multiple_of(start + which * (size // 2), 16), size // 2)

    def take(w, role, which, k=0):
        shard = (u_w, v_w, mix_w, up_w, down_w)[w]
        size, start = share[role], role * share[0]
        if w == 4:
            wide = pl.ds(0, width) if which is None else pl.ds(k * cut, cut)
            return shard.at[slab(size, which, start), wide]
        tall = shard.shape[0]
        cols = slice(None) if w < 3 else pl.ds(start, size)
        if which is None:
            return shard.at[:, cols]
        return shard.at[half(tall // 2 // parts[w], parts[w] * which + k), cols]

    def put(w, role, source, which, k=0):
        n, size = parts[w], share[role]
        if w == 4:
            wide = pl.ds(0, width) if which is None else pl.ds(k * cut, cut)
            return dng.at[source, slab(size, which), wide]
        whole, tall = ((uvg, ur), (uvg, ur), (mg, mr), (upg, pr))[w]
        cols = pl.ds(w * da, da) if w < 2 else slice(None) if w < 3 else pl.ds(0, size)
        if which is None:
            return whole.at[half(tall, source), cols]
        return whole.at[half(tall // 2 // n, n * (2 * source + which) + k), cols]

    def z_piece(w, role, dest, k):
        return remote(
            take(w, role, y, k), put(w, role, z, y, k), z_send.at[lane(w, k), dest],
            z_recv.at[lane(w, k), z], (y, dest, t),
        )

    def z_start(w, role, dest, ks=None):
        for k in range(parts[w]) if ks is None else ks:
            z_piece(w, role, dest, k).start()

    def y_piece(w, role, source, k):
        ref = put(w, role, source, y, k)
        return remote(ref, ref, y_send.at[lane(w, k), source], y_recv.at[lane(w, k), source], to_y)

    def y_arrived(w, role, source, k):
        ref = put(w, role, source, 1 - y, k)
        remote(
            ref, ref, y_send.at[lane(w, k), source], y_recv.at[lane(w, k), source], to_y
        ).wait_recv()

    def y_all(w, role):
        for o in others:
            for k in range(parts[w]):
                y_arrived(w, role, o, k)

    def relay(w, role, source, k):
        ref = put(w, role, source, y, k)
        remote(
            ref, ref, z_send.at[lane(w, k), source], z_recv.at[lane(w, k), source], (y, source, t)
        ).wait_recv()
        y_piece(w, role, source, k).start()

    def relays(w, role, source, ks=None):
        for k in range(parts[w]) if ks is None else ks:
            relay(w, role, source, k)

    def hop(w, source, way, own=False):
        ref = put(w, 0, source, y)
        return remote(
            take(w, 0, y) if own else ref, ref, h_send.at[w, source, way],
            z_recv.at[lane(w, 0), source], (y, z + 1 - 2 * way, t),
        )

    last = z_count - 1
    goes_on = (z < last, z > 0)

    def chain(w, distance):
        for way in range(2):
            source = z - distance if way == 0 else z + distance

            @pl.when(source >= 0 if way == 0 else source <= last)
            def _():
                hop(w, source, way).wait_recv()

                @pl.when(goes_on[way])
                def _():
                    hop(w, source, way).start()

                y_piece(w, 0, source, 0).start()

    def chain_pair(w):
        way = 1 - q
        hop(w, pair, way).wait_recv()
        hop(w, pair, way).start()
        y_piece(w, 0, pair, 0).start()

    def chain_facing(w):
        way = q
        hop(w, facing, way).wait_recv()
        hop(w, facing, way).start()
        y_piece(w, 0, facing, 0).start()

    def own_copies(w, role):
        return [
            pltpu.make_async_copy(
                take(w, role, None), put(w, role, z, None), l_sem.at[w]
            )
        ]

    def gather_copy(a, h, n):
        p, s, where = (
            (q, t, to_z), (q, t, to_x), (q, t, to_c), (1 - q, t, to_x), (1 - q, t, to_c),
            (q, t_chip, to_c), (1 - q, t_chip, to_c),
        )[n]
        ref = piece(a, h, p, s)
        return remote(ref, ref, a_send.at[a, h, n], a_recv.at[a, h, n], where)

    def gather_arrived(a, h, n):
        p, s, where = (
            (1 - q, t, to_z), (q, t_chip, to_x), (q, t_core, to_c), (1 - q, t_chip, to_x),
            (1 - q, t_core, to_c), (q, 3 - t, to_c), (1 - q, 3 - t, to_c),
        )[n]
        ref = piece(a, h, p, s)
        return remote(ref, ref, a_send.at[a, h, n], a_recv.at[a, h, n], where)

    def piece(a, h, p, s):
        if a == 0:
            return xg.at[s, pl.ds(h * step, step), :]
        return gat.at[s, h] if a == 1 else mid.at[p, s, pl.ds(h * step, step)]

    def gather_start(a, h):
        for n in (1, 2, 0)[: 3 if a == 2 else 2]:
            gather_copy(a, h, n).start()

    def gather_pair(a, h):
        gather_arrived(a, h, 0).wait_recv()
        gather_copy(a, h, 3).start()
        gather_copy(a, h, 4).start()

    def gather_rest(a, h):
        gather_arrived(a, h, 1).wait_recv()
        gather_copy(a, h, 5).start()
        if a == 2:
            gather_arrived(a, h, 3).wait_recv()
            gather_copy(a, h, 6).start()
        for n in (2, 4, 5, 6) if a == 2 else (2, 5):
            gather_arrived(a, h, n).wait_recv()

    chunks = rows // step
    inner = jnp.logical_and(z > 0, z < last)

    own_tok = pltpu.make_async_copy(tok, xg.at[t], l_sem.at[5])
    own_tok.start()
    def hop_own(w):
        for way in range(2):
            @pl.when(goes_on[way])
            def _():
                hop(w, z, way, True).start()

    hop_own(0)
    hop_own(1)
    own_tok.wait()
    for h in range(chunks):
        gather_start(0, h)
    def scaled(pieces, gain):
        total = pieces[0].shape[0]
        sums = jnp.zeros((total, 1), f32)
        for piece in pieces:
            sums += jnp.sum(piece * piece, axis=-1, keepdims=True)
        count = sum(piece.shape[1] for piece in pieces)
        scale = lax.rsqrt(sums / count + EPS)
        at = 0
        res = []
        for piece in pieces:
            wide = piece.shape[1]
            res.append((piece * scale * gain[:, at : at + wide]).astype(bf16))
            at += wide
        return jnp.concatenate(res, axis=1)

    small = 64
    per_part = step // small
    gain_one = gain1[...].astype(f32).reshape(1, -1)
    gain_two = gain2[...].astype(f32).reshape(1, -1)

    def norm_one(h):
        def loop(i, carry):
            here = pl.ds(pl.multiple_of(h * step + i * small, small), small)
            norm[here, :] = scaled([xg[s, here, :].astype(f32) for s in range(4)], gain_one)
            return carry

        lax.fori_loop(0, per_part, loop, 0)

    blk = spat.shape[1]
    lower = lax.broadcasted_iota(jnp.int32, (blk, blk), 0) >= lax.broadcasted_iota(
        jnp.int32, (blk, blk), 1
    )
    eye = lax.broadcasted_iota(jnp.int32, (blk, blk), 0) == lax.broadcasted_iota(
        jnp.int32, (blk, blk), 1
    )
    mixers, shifts, gains = [], [], []
    for g in range(da // gw):
        mixers.append(jnp.where(lower, spat[g].astype(f32), 0.0).astype(bf16))
        column = jnp.where(eye, bias[g : g + 1, :].astype(f32), 0.0)
        shifts.append(jnp.sum(column, axis=1, keepdims=True))
        gains.append(ggain[g : g + 1, :].astype(f32))

    def mix_rows(h):
        both = jnp.dot(norm[pl.ds(h * step, step), :], uvg[...], preferred_element_type=f32)
        both = jax.nn.gelu(both)
        u_act = both[:, :da].astype(bf16).astype(f32)
        for g in range(da // gw):
            cols = slice(g * gw, (g + 1) * gw)
            v_act = both[:, da + g * gw : da + (g + 1) * gw]
            v_n = (
                v_act
                * lax.rsqrt(jnp.mean(v_act * v_act, axis=-1, keepdims=True) + EPS)
                * gains[g]
            ).astype(bf16)
            for b in range(step // blk):
                part = slice(b * blk, (b + 1) * blk)
                mixed = jnp.dot(mixers[g], v_n[part], preferred_element_type=f32) + shifts[g]
                gat[t, h, part, cols] = (u_act[part, cols] * mixed).astype(bf16)

    def middle_rows(h):
        left = jnp.concatenate([gat[k, h] for k in range(4)], axis=1)
        value = jnp.dot(left, mg[...], preferred_element_type=f32)
        value += tok[pl.ds(h * step, step), :].astype(f32)
        mid[q, t, pl.ds(h * step, step)] = value.astype(bf16)

    def norm_two(h):
        def loop(i, carry):
            p, r = i // per_part, pl.multiple_of(lax.rem(i, per_part) * small, small)
            here = pl.ds(pl.multiple_of(h * step + r, small), small)
            pieces = [mid[p, k, here, :].astype(f32) for k in range(4)]
            at = pl.multiple_of((p * chunks + h) * step + r, small)
            norm[pl.ds(at, small), :] = scaled(pieces, gain_two)
            return carry

        lax.fori_loop(0, 2 * per_part, loop, 0)

    def up_rows(h, role):
        size = share[role]

        def loop(i, carry):
            here = pl.ds(pl.multiple_of((i * chunks + h) * step, step), step)
            pre = jnp.dot(norm[here, :], upg[:, :size], preferred_element_type=f32)
            hid[here, :size] = jnp.square(jax.nn.relu(pre)).astype(bf16)
            return carry

        lax.fori_loop(0, 2, loop, 0)

    def part(quarter, k, p, role):
        size, side = share[role], slice(k * col, (k + 1) * col)
        return jnp.dot(
            hid[half_rows(p), :size], dng[quarter, :size, side], preferred_element_type=f32
        )

    def half_rows(p):
        return pl.ds(pl.multiple_of(p * rows, rows), rows)

    def core_copy(n, k):
        return remote(
            c_out.at[n, k], c_in.at[n, k], c_send.at[n, k], c_recv.at[n, k], to_c
        )

    wide_n, slim_n = c, 1 - c
    own_wide = x == c

    def wide_x(k):
        return remote(c_in.at[wide_n, k], x_in.at[k], s_send.at[k], s_recv.at[k], to_x)

    def wide_z(k):
        return remote(z_out.at[k], z_in.at[k], r_send.at[k], r_recv.at[k], to_z)

    def slim_z(k):
        return remote(
            c_in.at[slim_n, k, half_rows(1 - q)], z_part.at[k], p_send.at[k], p_recv.at[k], to_z
        )

    def slim_x(k):
        return remote(x_out.at[k], x_part.at[k], o_send.at[k], o_recv.at[k], to_x)

    def down(quarter, k, role):
        n = quarter // 2
        mine = lax.rem(quarter, 2) == c

        @pl.when(jnp.logical_not(mine))
        def _():
            def loop(p, carry):
                c_out[n, k, half_rows(p), :] = part(quarter, k, p, role).astype(bf16)
                return carry

            lax.fori_loop(0, 2, loop, 0)
            core_copy(n, k).start()

        @pl.when(mine)
        def _():
            def loop(p, carry):
                acc[half_rows(p), :] = part(quarter, k, p, role)
                return carry

            lax.fori_loop(0, 2, loop, 0)
            core_copy(n, k).wait_recv()

            def add(b, carry):
                here = pl.ds(pl.multiple_of(b * small, small), small)
                value = acc[here, :] + c_in[n, k, here, :].astype(f32)
                c_in[n, k, here, :] = value.astype(bf16)
                return carry

            lax.fori_loop(0, 2 * rows // small, add, 0)

            @pl.when((n == wide_n) & jnp.logical_not(own_wide))
            def _():
                wide_x(k).start()

            @pl.when(n == slim_n)
            def _():
                slim_z(k).start()

    sides = range(cols)

    def in_rows(run):
        def loop(b, carry):
            run(
                pl.ds(pl.multiple_of(b * small, small), small),
                pl.ds(pl.multiple_of((1 - q) * rows + b * small, small), small),
                pl.ds(pl.multiple_of(q * rows + b * small, small), small),
            )
            return carry

        lax.fori_loop(0, rows // small, loop, 0)

    def meet(role):
        @pl.when(own_wide)
        def _():
            for k in sides:
                wide_x(k).wait_recv()

                def run(here, theirs, ours):
                    value = c_in[wide_n, k, theirs, :].astype(f32)
                    value += x_in[k, theirs, :].astype(f32)
                    z_out[k, here, :] = value.astype(bf16)

                in_rows(run)
                wide_z(k).start()

    every = range(cuts)

    def mixer():
        for w in range(2):
            for copy in own_copies(w, 0):
                copy.wait()
            y_all(w, 0)
        for h in range(chunks):
            mix_rows(h)
            gather_start(1, h)

    def middle():
        for copy in own_copies(2, 0):
            copy.wait()
        y_all(2, 0)
        for h in range(chunks):
            gather_rest(1, h)
            middle_rows(h)
            gather_start(2, h)

    def up_ready(role):
        for copy in own_copies(3, role):
            copy.wait()
        y_all(3, role)
        for copy in own_copies(4, role):
            copy.wait()

    def downs(role, source, ks=None):
        per = cuts // cols
        for k in sides if ks is None else ks:
            for i in range(per):
                y_arrived(4, role, source, k * per + i)
            down(source, k, role)

    def start(role):
        for w in range(5):
            for copy in own_copies(w, role):
                copy.start()

    @pl.when(jnp.logical_not(inner))
    def _():
        hop_own(2)
        start(0)
        z_start(3, 1, pair)
        z_start(3, 1, across)
        for w in range(2):
            chain(w, 1)
        for h in range(chunks):
            gather_rest(0, h)
            norm_one(h)
        for w in range(2):
            chain(w, 2)
        chain(2, 1)
        for w in range(2):
            chain(w, 3)
        chain(2, 2)
        chain(2, 3)
        mixer()
        middle()
        z_start(4, 1, across, every[:1])
        z_start(3, 0, facing)
        z_start(4, 1, pair)
        z_start(4, 0, facing)
        z_start(4, 1, across, every[1:])
        relays(3, 0, pair)
        gather_pair(2, 0)
        gather_pair(2, 1)
        gather_rest(2, 0)
        norm_two(0)
        relay(3, 0, facing, 0)
        gather_rest(2, 1)
        norm_two(1)
        relay(3, 0, facing, 1)
        relays(3, 0, across)
        relay(4, 0, across, 0)
        relay(4, 0, across, 1)
        up_ready(0)
        relay(4, 0, facing, 0)
        relay(4, 0, facing, 1)
        up_rows(0, 0)
        relay(4, 0, facing, 2)
        relay(4, 0, facing, 3)
        up_rows(1, 0)
        relay(4, 0, pair, 0)
        down(z, 0, 0)
        relay(4, 0, pair, 1)
        down(z, 1, 0)
        downs(0, across, sides[:1])
        relay(4, 0, pair, 2)
        downs(0, facing)
        relay(4, 0, across, 2)
        relay(4, 0, across, 3)
        relay(4, 0, pair, 3)
        downs(0, pair)
        downs(0, across, sides[1:])
        meet(0)

    @pl.when(inner)
    def _():
        start(1)
        for w in range(2):
            chain_pair(w)
            chain_facing(w)
        hop_own(2)
        chain_pair(2)
        z_start(3, 1, facing)
        z_start(4, 1, facing, every[:1])
        z_start(3, 0, across)
        z_start(4, 0, across)
        z_start(4, 1, facing, every[1:])
        for w in range(2):
            chain(w, 2)
        chain_facing(2)
        for h in range(chunks):
            gather_rest(0, h)
            norm_one(h)
        chain(2, 2)
        z_start(3, 0, pair)
        relays(3, 1, pair)
        mixer()
        relay(3, 1, across, 0)
        middle()
        z_start(4, 0, pair)
        relay(3, 1, across, 1)
        relay(3, 1, facing, 0)
        relay(3, 1, facing, 1)
        gather_pair(2, 0)
        gather_pair(2, 1)
        relay(4, 1, facing, 0)
        relay(4, 1, across, 0)
        gather_rest(2, 0)
        norm_two(0)
        gather_rest(2, 1)
        norm_two(1)
        relay(4, 1, pair, 0)
        up_ready(1)
        relay(4, 1, pair, 1)
        up_rows(0, 1)
        relay(4, 1, pair, 2)
        up_rows(1, 1)
        relay(4, 1, pair, 3)
        down(z, 0, 1)
        down(z, 1, 1)
        downs(1, pair)
        relay(4, 1, across, 1)
        relay(4, 1, across, 2)
        relay(4, 1, across, 3)
        relay(4, 1, facing, 1)
        downs(1, across)
        relays(4, 1, facing, every[2:])
        meet(1)
        downs(1, facing)

    def result(value, k, here):
        side = slice(k * col, (k + 1) * col)
        out[here, side] = (value + residual(here, side)).astype(bf16)

    def residual(here, side):
        return mid[q, t, here, side].astype(f32)

    @pl.when(own_wide)
    def _():
        for k in sides:
            slim_z(k).wait_recv()

            def run(here, theirs, ours):
                value = c_in[slim_n, k, ours, :].astype(f32) + z_part[k, here, :].astype(f32)
                x_out[k, here, :] = value.astype(bf16)

            in_rows(run)
            slim_x(k).start()
        for k in sides:
            wide_z(k).wait_recv()

            def run(here, theirs, ours):
                value = c_in[wide_n, k, ours, :].astype(f32) + x_in[k, ours, :].astype(f32)
                result(value + z_in[k, here, :].astype(f32), k, here)

            in_rows(run)
        for k in sides:
            wide_z(k).wait_send()
            slim_x(k).wait_send()

    @pl.when(jnp.logical_not(own_wide))
    def _():
        for k in sides:
            slim_z(k).wait_recv()
            slim_x(k).wait_recv()

            def run(here, theirs, ours):
                value = c_in[slim_n, k, ours, :].astype(f32) + z_part[k, here, :].astype(f32)
                result(value + x_part[k, here, :].astype(f32), k, here)

            in_rows(run)
        for k in sides:
            wide_x(k).wait_send()

    def drain(role):
        for w in range(5):
            for o, other in ((across, 1 - role), (facing, role), (pair, 1 - role)):
                for k in range(parts[w]):
                    if w > 2:
                        z_piece(w, other, o, k).wait_send()
                    y_piece(w, role, o, k).wait_send()

    @pl.when(jnp.logical_not(inner))
    def _():
        drain(0)

    @pl.when(inner)
    def _():
        drain(1)

    for w in range(3):
        for source in range(z_count):
            for way in range(2):
                came = source <= z if way == 0 else source >= z

                @pl.when(came & goes_on[way])
                def _():
                    hop(w, source, way).wait_send()

    for h in range(chunks):
        for a in range(3):
            for n in range(7) if a == 2 else (1, 2, 5):
                gather_copy(a, h, n).wait_send()
    for k in sides:
        for n in range(2):
            core_copy(n, k).wait_send()
        slim_z(k).wait_send()


def fused(tokens, first_gain, u_proj, v_proj, group_gain, spatial, spatial_bias, mix_proj,
          second_gain, up_proj, down_proj):
    rows, width = tokens.shape
    both, wide, da = 2 * rows, second_gain.shape[0], u_proj.shape[1]
    vmem, bf16, dma = pltpu.VMEM, jnp.bfloat16, pltpu.SemaphoreType.DMA
    spec = pl.BlockSpec(memory_space=pltpu.VMEM)
    ff = up_proj.shape[1] // 16 * 9
    step = 256
    chunks = rows // step
    cuts = 4
    cols = 2
    col = width // cols
    return pl.pallas_call(
        functools.partial(fused_kernel, step, cuts),
        out_shape=jax.ShapeDtypeStruct(tokens.shape, tokens.dtype),
        in_specs=[spec] * 11,
        out_specs=spec,
        scratch_shapes=[
            vmem((4, rows, width), bf16),
            vmem((wide, 2 * da), bf16),
            vmem((4 * mix_proj.shape[0], width), bf16),
            vmem((wide, ff), bf16),
            vmem((4, ff, width), bf16),
            vmem((both, wide), bf16),
            vmem((4, chunks, step, da), bf16),
            vmem((2, 4, rows, width), bf16),
            vmem((both, ff), bf16),
            vmem((2, cols, both, col), bf16),
            vmem((2, cols, both, col), bf16),
            vmem((cols, rows, col), bf16),
            vmem((cols, rows, col), bf16),
            vmem((cols, rows, col), bf16),
            vmem((cols, both, col), bf16),
            vmem((cols, rows, col), bf16),
            vmem((cols, rows, col), bf16),
            vmem((both, col), jnp.float32),
            dma((3, 4, 2)),
            dma((5 + cuts, 4)), dma((5 + cuts, 4)), dma((5 + cuts, 4)), dma((5 + cuts, 4)),
            dma((6,)),
            dma((3, chunks, 7)), dma((3, chunks, 7)),
            dma((2, cols)), dma((2, cols)), dma((cols,)), dma((cols,)), dma((cols,)),
            dma((cols,)), dma((cols,)), dma((cols,)), dma((cols,)), dma((cols,)),
        ],
        compiler_params=pltpu.CompilerParams(
            collective_id=0, has_side_effects=True, vmem_limit_bytes=64 * 1024 * 1000
        ),
    )(
        tokens, first_gain, u_proj, v_proj, group_gain, spatial, spatial_bias, mix_proj,
        second_gain, up_proj, down_proj,
    )


def layer_part(axes, *args):
    tokens, group_gain, spatial = args[0], args[4], args[5]
    fits = (
        axes["grp"] == 2
        and axes["fs"] == 4
        and axes["tp"] == 4
        and group_gain.shape[0] == 2
        and group_gain.shape[1] % 128 == 0
        and tokens.shape[0] % 256 == 0
        and tokens.shape[1] % 256 == 0
        and tokens.shape[1] == args[10].shape[1]
        and 256 % spatial.shape[1] == 0
        and args[9].shape[1] % 2048 == 0
    )
    return fused(*args) if fits else per_device(*args)


def solution(mesh):
    return jax.shard_map(
        functools.partial(layer_part, dict(mesh.shape)),
        mesh=mesh,
        in_specs=(
            P(("grp", "fs"), "tp"),
            P(),
            P("fs", "tp"),
            P("fs", "tp"),
            P("tp", None),
            P("tp", None, None),
            P("tp", None),
            P("fs", "tp"),
            P(),
            P("fs", "tp"),
            P("tp", "fs"),
        ),
        out_specs=P(("grp", "fs"), "tp"),
        check_vma=False,
    )
```

```python
import functools

import jax
import jax.numpy as jnp
from jax import lax
from jax.experimental import pallas as pl
from jax.experimental.pallas import tpu as pltpu
from jax.sharding import PartitionSpec as P

EPS = 1e-06


def rms_scale(values, gain_vec):
    mean_sq = jnp.mean(values * values, axis=-1, keepdims=True)
    return values * lax.rsqrt(mean_sq + EPS) * gain_vec.astype(jnp.float32)


def per_device(
    tokens,
    first_gain,
    u_proj,
    v_proj,
    group_gain,
    spatial,
    spatial_bias,
    mix_proj,
    second_gain,
    up_proj,
    down_proj,
):
    whole_rows = lax.all_gather(tokens, "tp", axis=1, tiled=True)
    row_count = whole_rows.shape[0]
    normed_rows = rms_scale(whole_rows.astype(jnp.float32), first_gain).astype(jnp.bfloat16)
    local_width = u_proj.shape[1]
    column_part = normed_rows
    u_pre = jnp.dot(
        column_part,
        lax.all_gather(u_proj, "fs", axis=0, tiled=True),
        preferred_element_type=jnp.float32,
    )
    v_pre = jnp.dot(
        column_part,
        lax.all_gather(v_proj, "fs", axis=0, tiled=True),
        preferred_element_type=jnp.float32,
    )
    u_act = jax.nn.gelu(u_pre).astype(jnp.bfloat16)
    local_groups = group_gain.shape[0]
    group_width = group_gain.shape[1]
    v_groups = jax.nn.gelu(v_pre).reshape(row_count, local_groups, group_width)
    v_normed = rms_scale(v_groups, group_gain).astype(jnp.bfloat16)
    block_len = spatial.shape[1]
    block_view = v_normed.reshape(row_count // block_len, block_len, local_groups, group_width)
    causal_mask = jnp.tril(jnp.ones((block_len, block_len), jnp.bool_))
    masked_weights = jnp.where(causal_mask[None], spatial, jnp.zeros_like(spatial))
    mixed_vals = jnp.einsum(
        "gts,nsgd->ntgd", masked_weights, block_view, preferred_element_type=jnp.float32
    )
    mixed_vals = mixed_vals + spatial_bias.astype(jnp.float32).T[None, :, :, None]
    gated_vals = (u_act.astype(jnp.float32) * mixed_vals.reshape(row_count, local_width)).astype(
        jnp.bfloat16
    )
    gated_whole = lax.all_gather(gated_vals, "tp", axis=1, tiled=True)
    column_part = gated_whole
    mix_vals = jnp.dot(
        column_part,
        lax.all_gather(mix_proj, "fs", axis=0, tiled=True),
        preferred_element_type=jnp.float32,
    )
    mid_stream = (tokens.astype(jnp.float32) + mix_vals).astype(jnp.bfloat16)
    mid_whole = lax.all_gather(mid_stream, "tp", axis=1, tiled=True)
    normed_two = rms_scale(mid_whole.astype(jnp.float32), second_gain).astype(jnp.bfloat16)
    column_part = normed_two
    pre_act = jnp.dot(
        column_part,
        lax.all_gather(up_proj, "fs", axis=0, tiled=True),
        preferred_element_type=jnp.float32,
    )
    hidden_act = jnp.square(jax.nn.relu(pre_act)).astype(jnp.bfloat16)
    down_terms = jnp.dot(
        hidden_act,
        lax.all_gather(down_proj, "fs", axis=1, tiled=True),
        preferred_element_type=jnp.float32,
    )
    down_sum = lax.psum_scatter(
        down_terms.astype(jnp.bfloat16), "tp", scatter_dimension=1, tiled=True
    ).astype(jnp.float32)
    return (mid_stream.astype(jnp.float32) + down_sum).astype(jnp.bfloat16)


def remote(src, dst, send, recv, where):
    return pltpu.make_async_remote_copy(
        src_ref=src,
        dst_ref=dst,
        send_sem=send,
        recv_sem=recv,
        device_id=where,
        device_id_type=pl.DeviceIdType.MESH,
    )


def fused_kernel(
    row_step, piece_cuts,
    tok, gain1, u_w, v_w, ggain, spat, bias, mix_w, gain2, up_w, down_w,
    out,
    xg, uvg, mg, upg, dng, norm, gat, mid, hid, c_out, c_in, z_out, z_in, z_part, x_in, x_out, x_part,
    acc,
    h_send, z_send, z_recv, y_send, y_recv, l_sem, a_send, a_recv, c_send, c_recv, r_send,
    r_recv, s_send, s_recv, p_send, p_recv, o_send, o_recv,
):
    y, z, t = lax.axis_index("grp"), lax.axis_index("fs"), lax.axis_index("tp")
    q, c, x = lax.rem(z, 2), lax.rem(t, 2), t // 2
    z_pair = z + 1 - 2 * q
    t_core, t_chip = t + 1 - 2 * c, lax.rem(t + 2, 4)
    to_y, to_z = (1 - y, z, t), (y, z_pair, t)
    to_c, to_x = (y, z, t_core), (y, z, t_chip)
    across, facing, pair = others = (lax.rem(z + 2, 4), 3 - z, z_pair)
    rows, width = tok.shape
    step, z_count = row_step, dng.shape[0]
    f32, bf16 = jnp.float32, jnp.bfloat16

    own_tok = pltpu.make_async_copy(tok, xg.at[t], l_sem.at[5])
    own_tok.start()
    barrier = pltpu.get_barrier_semaphore()
    for where in (to_y, to_c, to_x) + tuple((y, o, t) for o in others):
        pl.semaphore_signal(
            barrier, inc=1, device_id=where, device_id_type=pl.DeviceIdType.MESH
        )
    pl.semaphore_wait(barrier, 6)

    gw, da = ggain.shape[1], u_w.shape[1]
    ur, mr, pr = u_w.shape[0], mix_w.shape[0], up_w.shape[0]
    ff, inner_ff = up_w.shape[1], hid.shape[1]
    share = (ff - inner_ff, inner_ff)

    def half(size, which):
        return pl.ds(pl.multiple_of(which * size, size), size)

    cuts, cut = piece_cuts, width // piece_cuts
    cols, col = c_out.shape[1], c_out.shape[3]
    parts = (1, 1, 1, 2, cuts)

    def lane(w, k):
        return sum(parts[:w]) + k

    def slab(size, which, start=0):
        if which is None:
            return pl.ds(start, size)
        return pl.ds(pl.multiple_of(start + which * (size // 2), 16), size // 2)

    def take(w, role, which, k=0):
        shard = (u_w, v_w, mix_w, up_w, down_w)[w]
        size, start = share[role], role * share[0]
        if w == 4:
            wide = pl.ds(0, width) if which is None else pl.ds(k * cut, cut)
            return shard.at[slab(size, which, start), wide]
        tall = shard.shape[0]
        cols = slice(None) if w < 3 else pl.ds(start, size)
        if which is None:
            return shard.at[:, cols]
        return shard.at[half(tall // 2 // parts[w], parts[w] * which + k), cols]

    def put(w, role, source, which, k=0):
        n, size = parts[w], share[role]
        if w == 4:
            wide = pl.ds(0, width) if which is None else pl.ds(k * cut, cut)
            return dng.at[source, slab(size, which), wide]
        whole, tall = ((uvg, ur), (uvg, ur), (mg, mr), (upg, pr))[w]
        cols = pl.ds(w * da, da) if w < 2 else slice(None) if w < 3 else pl.ds(0, size)
        if which is None:
            return whole.at[half(tall, source), cols]
        return whole.at[half(tall // 2 // n, n * (2 * source + which) + k), cols]

    def z_piece(w, role, dest, k):
        return remote(
            take(w, role, y, k), put(w, role, z, y, k), z_send.at[lane(w, k) - 3, dest],
            z_recv.at[lane(w, k), z], (y, dest, t),
        )

    def z_start(w, role, dest, ks=None):
        for k in range(parts[w]) if ks is None else ks:
            z_piece(w, role, dest, k).start()

    def y_piece(w, role, source, k):
        ref = put(w, role, source, y, k)
        return remote(ref, ref, y_send.at[lane(w, k), source], y_recv.at[lane(w, k), source], to_y)

    def y_arrived(w, role, source, k):
        ref = put(w, role, source, 1 - y, k)
        remote(
            ref, ref, y_send.at[lane(w, k), source], y_recv.at[lane(w, k), source], to_y
        ).wait_recv()

    def y_all(w, role):
        for o in others:
            for k in range(parts[w]):
                y_arrived(w, role, o, k)

    def relay(w, role, source, k):
        ref = put(w, role, source, y, k)
        remote(
            ref, ref, z_send.at[lane(w, k) - 3, source], z_recv.at[lane(w, k), source], (y, source, t)
        ).wait_recv()
        y_piece(w, role, source, k).start()

    def relays(w, role, source, ks=None):
        for k in range(parts[w]) if ks is None else ks:
            relay(w, role, source, k)

    def hop(w, source, way, own=False):
        ref = put(w, 0, source, y)
        return remote(
            take(w, 0, y) if own else ref, ref, h_send.at[w, source, way],
            z_recv.at[lane(w, 0), source], (y, z + 1 - 2 * way, t),
        )

    last = z_count - 1
    goes_on = (z < last, z > 0)

    def chain(w, distance):
        for way in range(2):
            source = z - distance if way == 0 else z + distance

            @pl.when(source >= 0 if way == 0 else source <= last)
            def _():
                hop(w, source, way).wait_recv()

                @pl.when(goes_on[way])
                def _():
                    hop(w, source, way).start()

                y_piece(w, 0, source, 0).start()

    def chain_pair(w):
        way = 1 - q
        hop(w, pair, way).wait_recv()
        hop(w, pair, way).start()
        y_piece(w, 0, pair, 0).start()

    def chain_facing(w):
        way = q
        hop(w, facing, way).wait_recv()
        hop(w, facing, way).start()
        y_piece(w, 0, facing, 0).start()

    def own_copies(w, role):
        return [
            pltpu.make_async_copy(
                take(w, role, None), put(w, role, z, None), l_sem.at[w]
            )
        ]

    def link(a, n):
        return 6 + n if a == 2 else 3 * a + (1, 2, 5).index(n)

    def gather_copy(a, h, n):
        p, s, where = (
            (q, t, to_z), (q, t, to_x), (q, t, to_c), (1 - q, t, to_x), (1 - q, t, to_c),
            (q, t_chip, to_c), (1 - q, t_chip, to_c),
        )[n]
        ref = piece(a, h, p, s)
        return remote(ref, ref, a_send.at[link(a, n), h], a_recv.at[link(a, n), h], where)

    def gather_arrived(a, h, n):
        p, s, where = (
            (1 - q, t, to_z), (q, t_chip, to_x), (q, t_core, to_c), (1 - q, t_chip, to_x),
            (1 - q, t_core, to_c), (q, 3 - t, to_c), (1 - q, 3 - t, to_c),
        )[n]
        ref = piece(a, h, p, s)
        return remote(ref, ref, a_send.at[link(a, n), h], a_recv.at[link(a, n), h], where)

    def piece(a, h, p, s):
        if a == 0:
            return xg.at[s, pl.ds(h * step, step), :]
        return gat.at[s, h] if a == 1 else mid.at[p, s, pl.ds(h * step, step)]

    def gather_start(a, h):
        for n in (1, 2, 0)[: 3 if a == 2 else 2]:
            gather_copy(a, h, n).start()

    def gather_pair(a, h):
        gather_arrived(a, h, 0).wait_recv()
        gather_copy(a, h, 3).start()
        gather_copy(a, h, 4).start()

    def gather_rest(a, h):
        gather_arrived(a, h, 1).wait_recv()
        gather_copy(a, h, 5).start()
        if a == 2:
            gather_arrived(a, h, 3).wait_recv()
            gather_copy(a, h, 6).start()
        for n in (2, 4, 5, 6) if a == 2 else (2, 5):
            gather_arrived(a, h, n).wait_recv()

    chunks = rows // step
    inner = jnp.logical_and(z > 0, z < last)

    def hop_own(w):
        for way in range(2):
            @pl.when(goes_on[way])
            def _():
                hop(w, z, way, True).start()

    hop_own(0)
    hop_own(1)
    own_tok.wait()
    for h in range(chunks):
        gather_start(0, h)
    def scaled(pieces, gain):
        total = pieces[0].shape[0]
        sums = jnp.zeros((total, 1), f32)
        for piece in pieces:
            sums += jnp.sum(piece * piece, axis=-1, keepdims=True)
        count = sum(piece.shape[1] for piece in pieces)
        scale = lax.rsqrt(sums / count + EPS)
        at = 0
        res = []
        for piece in pieces:
            wide = piece.shape[1]
            res.append((piece * scale * gain[:, at : at + wide]).astype(bf16))
            at += wide
        return jnp.concatenate(res, axis=1)

    small = 64
    per_part = step // small
    gain_one = gain1[...].astype(f32).reshape(1, -1)
    gain_two = gain2[...].astype(f32).reshape(1, -1)

    def norm_one(h):
        def loop(i, carry):
            here = pl.ds(pl.multiple_of(h * step + i * small, small), small)
            norm[here, :] = scaled([xg[s, here, :].astype(f32) for s in range(4)], gain_one)
            return carry

        lax.fori_loop(0, per_part, loop, 0)

    blk = spat.shape[1]
    lower = lax.broadcasted_iota(jnp.int32, (blk, blk), 0) >= lax.broadcasted_iota(
        jnp.int32, (blk, blk), 1
    )
    eye = lax.broadcasted_iota(jnp.int32, (blk, blk), 0) == lax.broadcasted_iota(
        jnp.int32, (blk, blk), 1
    )
    mixers, shifts, gains = [], [], []
    for g in range(da // gw):
        mixers.append(jnp.where(lower, spat[g].astype(f32), 0.0).astype(bf16))
        column = jnp.where(eye, bias[g : g + 1, :].astype(f32), 0.0)
        shifts.append(jnp.sum(column, axis=1, keepdims=True))
        gains.append(ggain[g : g + 1, :].astype(f32))

    def mix_rows(h):
        both = jnp.dot(norm[pl.ds(h * step, step), :], uvg[...], preferred_element_type=f32)
        both = jax.nn.gelu(both)
        u_act = both[:, :da].astype(bf16).astype(f32)
        for g in range(da // gw):
            cols = slice(g * gw, (g + 1) * gw)
            v_act = both[:, da + g * gw : da + (g + 1) * gw]
            v_n = (
                v_act
                * lax.rsqrt(jnp.mean(v_act * v_act, axis=-1, keepdims=True) + EPS)
                * gains[g]
            ).astype(bf16)
            for b in range(step // blk):
                part = slice(b * blk, (b + 1) * blk)
                mixed = jnp.dot(mixers[g], v_n[part], preferred_element_type=f32) + shifts[g]
                gat[t, h, part, cols] = (u_act[part, cols] * mixed).astype(bf16)

    def middle_rows(h):
        left = jnp.concatenate([gat[k, h] for k in range(4)], axis=1)
        value = jnp.dot(left, mg[...], preferred_element_type=f32)
        value += xg[t, pl.ds(h * step, step), :].astype(f32)
        mid[q, t, pl.ds(h * step, step)] = value.astype(bf16)

    def norm_two(h):
        def loop(i, carry):
            p, r = i // per_part, pl.multiple_of(lax.rem(i, per_part) * small, small)
            here = pl.ds(pl.multiple_of(h * step + r, small), small)
            pieces = [mid[p, k, here, :].astype(f32) for k in range(4)]
            at = pl.multiple_of((p * chunks + h) * step + r, small)
            norm[pl.ds(at, small), :] = scaled(pieces, gain_two)
            return carry

        lax.fori_loop(0, 2 * per_part, loop, 0)

    def up_rows(h, role):
        size = share[role]

        def loop(i, carry):
            here = pl.ds(pl.multiple_of((i * chunks + h) * step, step), step)
            pre = jnp.dot(norm[here, :], upg[:, :size], preferred_element_type=f32)
            hid[here, :size] = jnp.square(jax.nn.relu(pre)).astype(bf16)
            return carry

        lax.fori_loop(0, 2, loop, 0)

    def part(quarter, k, p, role):
        size, side = share[role], slice(k * col, (k + 1) * col)
        return jnp.dot(
            hid[half_rows(p), :size], dng[quarter, :size, side], preferred_element_type=f32
        )

    def half_rows(p):
        return pl.ds(pl.multiple_of(p * rows, rows), rows)

    def core_copy(n, k):
        return remote(
            c_out.at[n, k], c_in.at[n, k], c_send.at[n, k], c_recv.at[n, k], to_c
        )

    wide_n, slim_n = c, 1 - c
    own_wide = x == c

    def wide_x(k):
        return remote(c_in.at[wide_n, k], x_in.at[k], s_send.at[k], s_recv.at[k], to_x)

    def wide_z(k):
        return remote(z_out.at[k], z_in.at[k], r_send.at[k], r_recv.at[k], to_z)

    def slim_z(k):
        return remote(
            c_in.at[slim_n, k, half_rows(1 - q)], z_part.at[k], p_send.at[k], p_recv.at[k], to_z
        )

    def slim_x(k):
        return remote(x_out.at[k], x_part.at[k], o_send.at[k], o_recv.at[k], to_x)

    def down(quarter, k, role):
        n = quarter // 2
        mine = lax.rem(quarter, 2) == c

        @pl.when(jnp.logical_not(mine))
        def _():
            def loop(p, carry):
                c_out[n, k, half_rows(p), :] = part(quarter, k, p, role).astype(bf16)
                return carry

            lax.fori_loop(0, 2, loop, 0)
            core_copy(n, k).start()

        @pl.when(mine)
        def _():
            def loop(p, carry):
                acc[half_rows(p), :] = part(quarter, k, p, role)
                return carry

            lax.fori_loop(0, 2, loop, 0)
            core_copy(n, k).wait_recv()

            def add(b, carry):
                here = pl.ds(pl.multiple_of(b * small, small), small)
                value = acc[here, :] + c_in[n, k, here, :].astype(f32)
                c_in[n, k, here, :] = value.astype(bf16)
                return carry

            lax.fori_loop(0, 2 * rows // small, add, 0)

            @pl.when((n == wide_n) & jnp.logical_not(own_wide))
            def _():
                wide_x(k).start()

            @pl.when(n == slim_n)
            def _():
                slim_z(k).start()

    sides = range(cols)
    low, high = sides[: cols // 2], sides[cols // 2 :]

    def in_rows(run):
        def loop(b, carry):
            run(
                pl.ds(pl.multiple_of(b * small, small), small),
                pl.ds(pl.multiple_of((1 - q) * rows + b * small, small), small),
                pl.ds(pl.multiple_of(q * rows + b * small, small), small),
            )
            return carry

        lax.fori_loop(0, rows // small, loop, 0)

    def meet(ks, fits=True):
        @pl.when(own_wide & fits)
        def _():
            for k in ks:
                wide_x(k).wait_recv()

                def run(here, theirs, ours):
                    value = c_in[wide_n, k, theirs, :].astype(f32)
                    value += x_in[k, theirs, :].astype(f32)
                    z_out[k, here, :] = value.astype(bf16)

                in_rows(run)
                wide_z(k).start()

    every = range(cuts)

    def mixer():
        for w in range(2):
            for copy in own_copies(w, 0):
                copy.wait()
            y_all(w, 0)
        for h in range(chunks):
            mix_rows(h)
            gather_start(1, h)

    def middle():
        for copy in own_copies(2, 0):
            copy.wait()
        y_all(2, 0)
        for h in range(chunks):
            gather_rest(1, h)
            middle_rows(h)
            gather_start(2, h)

    def up_ready(role):
        for copy in own_copies(3, role):
            copy.wait()
        y_all(3, role)
        for copy in own_copies(4, role):
            copy.wait()

    def downs(role, source, ks=None):
        per = cuts // cols
        for k in sides if ks is None else ks:
            for i in range(per):
                y_arrived(4, role, source, k * per + i)
            down(source, k, role)

    def last_downs(role, k):
        per = cuts // cols
        for source in (pair, across):
            for i in range(per):
                y_arrived(4, role, source, k * per + i)
        pair_first = lax.rem(pair, 2) != c
        down(jnp.where(pair_first, pair, across), k, role)
        down(jnp.where(pair_first, across, pair), k, role)

    def start(role):
        for w in range(5):
            for copy in own_copies(w, role):
                copy.start()

    @pl.when(jnp.logical_not(inner))
    def _():
        hop_own(2)
        start(0)
        z_start(3, 1, pair)
        z_start(3, 1, across)
        for w in range(2):
            chain(w, 1)
        for h in range(chunks):
            gather_rest(0, h)
            norm_one(h)
        for w in range(2):
            chain(w, 2)
        chain(2, 1)
        for w in range(2):
            chain(w, 3)
        chain(2, 2)
        chain(2, 3)
        mixer()
        middle()
        z_start(4, 1, across, every[:1])
        z_start(3, 0, facing)
        z_start(4, 1, pair)
        z_start(4, 0, facing)
        z_start(4, 1, across, every[1:])
        relays(3, 0, pair)
        gather_pair(2, 0)
        gather_pair(2, 1)
        gather_rest(2, 0)
        norm_two(0)
        relay(3, 0, facing, 0)
        gather_rest(2, 1)
        norm_two(1)
        relay(3, 0, facing, 1)
        relays(3, 0, across)
        relay(4, 0, across, 0)
        relay(4, 0, across, 1)
        up_ready(0)
        relay(4, 0, facing, 0)
        relay(4, 0, facing, 1)
        up_rows(0, 0)
        relay(4, 0, facing, 2)
        relay(4, 0, facing, 3)
        up_rows(1, 0)
        relay(4, 0, pair, 0)
        for k in low:
            down(z, k, 0)
        relay(4, 0, pair, 1)
        for k in high:
            down(z, k, 0)
        downs(0, across, low)
        relay(4, 0, pair, 2)
        downs(0, facing)
        relay(4, 0, across, 2)
        relay(4, 0, across, 3)
        relay(4, 0, pair, 3)
        downs(0, pair, low)
        meet(low)
        for k in high:
            last_downs(0, k)
        meet(high)

    @pl.when(inner)
    def _():
        start(1)
        for w in range(2):
            chain_pair(w)
            chain_facing(w)
        hop_own(2)
        chain_pair(2)
        z_start(3, 1, facing)
        z_start(4, 1, facing, every[:1])
        z_start(3, 0, across)
        z_start(4, 0, across)
        z_start(4, 1, facing, every[1:])
        for w in range(2):
            chain(w, 2)
        chain_facing(2)
        for h in range(chunks):
            gather_rest(0, h)
            norm_one(h)
        chain(2, 2)
        z_start(3, 0, pair)
        relays(3, 1, pair)
        mixer()
        relay(3, 1, across, 0)
        middle()
        z_start(4, 0, pair)
        relay(3, 1, across, 1)
        relay(3, 1, facing, 0)
        relay(3, 1, facing, 1)
        gather_pair(2, 0)
        gather_pair(2, 1)
        relay(4, 1, facing, 0)
        relay(4, 1, across, 0)
        gather_rest(2, 0)
        norm_two(0)
        gather_rest(2, 1)
        norm_two(1)
        relay(4, 1, pair, 0)
        up_ready(1)
        relay(4, 1, pair, 1)
        up_rows(0, 1)
        relay(4, 1, pair, 2)
        up_rows(1, 1)
        relay(4, 1, pair, 3)
        for k in low:
            down(z, k, 1)
        for k in high:
            down(z, k, 1)
        downs(1, pair)
        relay(4, 1, across, 1)
        relay(4, 1, across, 2)
        relay(4, 1, across, 3)
        downs(1, across, low)
        relay(4, 1, facing, 1)
        downs(1, across, high)
        relays(4, 1, facing, every[2:])
        meet(sides, t == pair)
        downs(1, facing)
        meet(sides, t == across)

    def result(value, k, here):
        side = slice(k * col, (k + 1) * col)
        out[here, side] = (value + residual(here, side)).astype(bf16)

    def residual(here, side):
        return mid[q, t, here, side].astype(f32)

    @pl.when(own_wide)
    def _():
        for k in sides:
            slim_z(k).wait_recv()

            def run(here, theirs, ours):
                value = c_in[slim_n, k, ours, :].astype(f32) + z_part[k, here, :].astype(f32)
                x_out[k, here, :] = value.astype(bf16)

            in_rows(run)
            slim_x(k).start()
        for k in sides:
            wide_z(k).wait_recv()

            def run(here, theirs, ours):
                value = c_in[wide_n, k, ours, :].astype(f32) + x_in[k, ours, :].astype(f32)
                result(value + z_in[k, here, :].astype(f32), k, here)

            in_rows(run)
        for k in sides:
            wide_z(k).wait_send()
            slim_x(k).wait_send()

    @pl.when(jnp.logical_not(own_wide))
    def _():
        for k in sides:
            slim_z(k).wait_recv()
            slim_x(k).wait_recv()

            def run(here, theirs, ours):
                value = c_in[slim_n, k, ours, :].astype(f32) + z_part[k, here, :].astype(f32)
                result(value + x_part[k, here, :].astype(f32), k, here)

            in_rows(run)
        for k in sides:
            wide_x(k).wait_send()

    def drain(role):
        for w in range(5):
            for o, other in ((across, 1 - role), (facing, role), (pair, 1 - role)):
                for k in range(parts[w]):
                    if w > 2:
                        z_piece(w, other, o, k).wait_send()
                    y_piece(w, role, o, k).wait_send()

    @pl.when(jnp.logical_not(inner))
    def _():
        drain(0)

    @pl.when(inner)
    def _():
        drain(1)

    for w in range(3):
        for source in range(z_count):
            for way in range(2):
                came = source <= z if way == 0 else source >= z

                @pl.when(came & goes_on[way])
                def _():
                    hop(w, source, way).wait_send()

    for h in range(chunks):
        for a in range(3):
            for n in range(7) if a == 2 else (1, 2, 5):
                gather_copy(a, h, n).wait_send()
    for k in sides:
        for n in range(2):
            core_copy(n, k).wait_send()
        slim_z(k).wait_send()


def fused(tokens, first_gain, u_proj, v_proj, group_gain, spatial, spatial_bias, mix_proj,
          second_gain, up_proj, down_proj):
    rows, width = tokens.shape
    both, wide, da = 2 * rows, second_gain.shape[0], u_proj.shape[1]
    vmem, bf16, dma = pltpu.VMEM, jnp.bfloat16, pltpu.SemaphoreType.DMA
    spec, far = (pl.BlockSpec(memory_space=m) for m in (pltpu.VMEM, pl.ANY))
    ff = up_proj.shape[1] // 16 * 9
    step = 256
    chunks = rows // step
    cuts = 4
    cols = 4
    col = width // cols
    return pl.pallas_call(
        functools.partial(fused_kernel, step, cuts),
        out_shape=jax.ShapeDtypeStruct(tokens.shape, tokens.dtype),
        in_specs=[far, spec, far, far, spec, spec, spec, far, spec, far, far],
        out_specs=spec,
        scratch_shapes=[
            vmem((4, rows, width), bf16),
            vmem((wide, 2 * da), bf16),
            vmem((4 * mix_proj.shape[0], width), bf16),
            vmem((wide, ff), bf16),
            vmem((4, ff, width), bf16),
            vmem((both, wide), bf16),
            vmem((4, chunks, step, da), bf16),
            vmem((2, 4, rows, width), bf16),
            vmem((both, ff), bf16),
            vmem((2, cols, both, col), bf16),
            vmem((2, cols, both, col), bf16),
            vmem((cols, rows, col), bf16),
            vmem((cols, rows, col), bf16),
            vmem((cols, rows, col), bf16),
            vmem((cols, both, col), bf16),
            vmem((cols, rows, col), bf16),
            vmem((cols, rows, col), bf16),
            vmem((both, col), jnp.float32),
            dma((3, 4, 2)),
            dma((2 + cuts, 4)), dma((5 + cuts, 4)), dma((5 + cuts, 4)), dma((5 + cuts, 4)),
            dma((6,)),
            dma((13, chunks)), dma((13, chunks)),
            dma((2, cols)), dma((2, cols)), dma((cols,)), dma((cols,)), dma((cols,)),
            dma((cols,)), dma((cols,)), dma((cols,)), dma((cols,)), dma((cols,)),
        ],
        compiler_params=pltpu.CompilerParams(
            collective_id=0, has_side_effects=True, vmem_limit_bytes=64 * 1024 * 1000
        ),
    )(
        tokens, first_gain, u_proj, v_proj, group_gain, spatial, spatial_bias, mix_proj,
        second_gain, up_proj, down_proj,
    )


def layer_part(axes, *args):
    tokens, group_gain, spatial = args[0], args[4], args[5]
    fits = (
        axes["grp"] == 2
        and axes["fs"] == 4
        and axes["tp"] == 4
        and group_gain.shape[0] == 2
        and group_gain.shape[1] % 128 == 0
        and tokens.shape[0] % 256 == 0
        and tokens.shape[1] % 256 == 0
        and tokens.shape[1] == args[10].shape[1]
        and 256 % spatial.shape[1] == 0
        and args[9].shape[1] % 2048 == 0
    )
    return fused(*args) if fits else per_device(*args)


def solution(mesh):
    return jax.shard_map(
        functools.partial(layer_part, dict(mesh.shape)),
        mesh=mesh,
        in_specs=(
            P(("grp", "fs"), "tp"),
            P(),
            P("fs", "tp"),
            P("fs", "tp"),
            P("tp", None),
            P("tp", None, None),
            P("tp", None),
            P("fs", "tp"),
            P(),
            P("fs", "tp"),
            P("tp", "fs"),
        ),
        out_specs=P(("grp", "fs"), "tp"),
        check_vma=False,
    )
```

```python
import functools

import jax
import jax.numpy as jnp
from jax import lax
from jax.experimental import pallas as pl
from jax.experimental.pallas import tpu as pltpu
from jax.sharding import PartitionSpec as P

EPS = 1e-06


def rms_scale(values, gain_vec):
    mean_sq = jnp.mean(values * values, axis=-1, keepdims=True)
    return values * lax.rsqrt(mean_sq + EPS) * gain_vec.astype(jnp.float32)


def per_device(
    tokens,
    first_gain,
    u_proj,
    v_proj,
    group_gain,
    spatial,
    spatial_bias,
    mix_proj,
    second_gain,
    up_proj,
    down_proj,
):
    whole_rows = lax.all_gather(tokens, "tp", axis=1, tiled=True)
    row_count = whole_rows.shape[0]
    normed_rows = rms_scale(whole_rows.astype(jnp.float32), first_gain).astype(jnp.bfloat16)
    local_width = u_proj.shape[1]
    column_part = normed_rows
    u_pre = jnp.dot(
        column_part,
        lax.all_gather(u_proj, "fs", axis=0, tiled=True),
        preferred_element_type=jnp.float32,
    )
    v_pre = jnp.dot(
        column_part,
        lax.all_gather(v_proj, "fs", axis=0, tiled=True),
        preferred_element_type=jnp.float32,
    )
    u_act = jax.nn.gelu(u_pre).astype(jnp.bfloat16)
    local_groups = group_gain.shape[0]
    group_width = group_gain.shape[1]
    v_groups = jax.nn.gelu(v_pre).reshape(row_count, local_groups, group_width)
    v_normed = rms_scale(v_groups, group_gain).astype(jnp.bfloat16)
    block_len = spatial.shape[1]
    block_view = v_normed.reshape(row_count // block_len, block_len, local_groups, group_width)
    causal_mask = jnp.tril(jnp.ones((block_len, block_len), jnp.bool_))
    masked_weights = jnp.where(causal_mask[None], spatial, jnp.zeros_like(spatial))
    mixed_vals = jnp.einsum(
        "gts,nsgd->ntgd", masked_weights, block_view, preferred_element_type=jnp.float32
    )
    mixed_vals = mixed_vals + spatial_bias.astype(jnp.float32).T[None, :, :, None]
    gated_vals = (u_act.astype(jnp.float32) * mixed_vals.reshape(row_count, local_width)).astype(
        jnp.bfloat16
    )
    gated_whole = lax.all_gather(gated_vals, "tp", axis=1, tiled=True)
    column_part = gated_whole
    mix_vals = jnp.dot(
        column_part,
        lax.all_gather(mix_proj, "fs", axis=0, tiled=True),
        preferred_element_type=jnp.float32,
    )
    mid_stream = (tokens.astype(jnp.float32) + mix_vals).astype(jnp.bfloat16)
    mid_whole = lax.all_gather(mid_stream, "tp", axis=1, tiled=True)
    normed_two = rms_scale(mid_whole.astype(jnp.float32), second_gain).astype(jnp.bfloat16)
    column_part = normed_two
    pre_act = jnp.dot(
        column_part,
        lax.all_gather(up_proj, "fs", axis=0, tiled=True),
        preferred_element_type=jnp.float32,
    )
    hidden_act = jnp.square(jax.nn.relu(pre_act)).astype(jnp.bfloat16)
    down_terms = jnp.dot(
        hidden_act,
        lax.all_gather(down_proj, "fs", axis=1, tiled=True),
        preferred_element_type=jnp.float32,
    )
    down_sum = lax.psum_scatter(
        down_terms.astype(jnp.bfloat16), "tp", scatter_dimension=1, tiled=True
    ).astype(jnp.float32)
    return (mid_stream.astype(jnp.float32) + down_sum).astype(jnp.bfloat16)


def remote(src, dst, send, recv, where):
    return pltpu.make_async_remote_copy(
        src_ref=src,
        dst_ref=dst,
        send_sem=send,
        recv_sem=recv,
        device_id=where,
        device_id_type=pl.DeviceIdType.MESH,
    )


def fused_kernel(
    row_step, piece_cuts,
    tok, far_gain1, u_w, v_w, far_ggain, far_spat, far_bias, mix_w, far_gain2, up_w, down_w,
    out,
    gain1, ggain, spat, bias, gain2,
    xg, uvg, mg, upg, dng, norm, gat, mid, hid, c_out, c_in, z_out, z_in, z_part, x_in, x_out, x_part,
    acc,
    h_send, z_send, z_recv, y_send, y_recv, l_sem, a_send, a_recv, c_send, c_recv, r_send,
    r_recv, s_send, s_recv, p_send, p_recv, o_send, o_recv,
):
    y, z, t = lax.axis_index("grp"), lax.axis_index("fs"), lax.axis_index("tp")
    q, c, x = lax.rem(z, 2), lax.rem(t, 2), t // 2
    z_pair = z + 1 - 2 * q
    t_core, t_chip = t + 1 - 2 * c, lax.rem(t + 2, 4)
    to_y, to_z = (1 - y, z, t), (y, z_pair, t)
    to_c, to_x = (y, z, t_core), (y, z, t_chip)
    across, facing, pair = others = (lax.rem(z + 2, 4), 3 - z, z_pair)
    rows, width = tok.shape
    step, z_count = row_step, dng.shape[0]
    f32, bf16 = jnp.float32, jnp.bfloat16

    own_tok = pltpu.make_async_copy(tok, xg.at[t], l_sem.at[5])
    own_tok.start()
    fetches = [
        pltpu.make_async_copy(held, near, l_sem.at[6 + i])
        for i, (held, near) in enumerate((
            (far_gain1, gain1), (far_ggain, ggain), (far_spat, spat), (far_bias, bias),
            (far_gain2, gain2),
        ))
    ]
    for fetch in fetches:
        fetch.start()
    barrier = pltpu.get_barrier_semaphore()
    for where in (to_y, to_c, to_x) + tuple((y, o, t) for o in others):
        pl.semaphore_signal(
            barrier, inc=1, device_id=where, device_id_type=pl.DeviceIdType.MESH
        )
    pl.semaphore_wait(barrier, 6)

    gw, da = ggain.shape[1], u_w.shape[1]
    ur, mr, pr = u_w.shape[0], mix_w.shape[0], up_w.shape[0]
    ff, inner_ff = up_w.shape[1], hid.shape[1]
    share = (ff - inner_ff, inner_ff)

    def half(size, which):
        return pl.ds(pl.multiple_of(which * size, size), size)

    cuts, cut = piece_cuts, width // piece_cuts
    cols, col = c_out.shape[1], c_out.shape[3]
    parts = (1, 1, 1, 2, cuts)

    def lane(w, k):
        return sum(parts[:w]) + k

    def slab(size, which, start=0):
        if which is None:
            return pl.ds(start, size)
        return pl.ds(pl.multiple_of(start + which * (size // 2), 16), size // 2)

    def take(w, role, which, k=0):
        shard = (u_w, v_w, mix_w, up_w, down_w)[w]
        size, start = share[role], role * share[0]
        if w == 4:
            wide = pl.ds(0, width) if which is None else pl.ds(k * cut, cut)
            return shard.at[slab(size, which, start), wide]
        tall = shard.shape[0]
        cols = slice(None) if w < 3 else pl.ds(start, size)
        if which is None:
            return shard.at[:, cols]
        return shard.at[half(tall // 2 // parts[w], parts[w] * which + k), cols]

    def put(w, role, source, which, k=0):
        n, size = parts[w], share[role]
        if w == 4:
            wide = pl.ds(0, width) if which is None else pl.ds(k * cut, cut)
            return dng.at[source, slab(size, which), wide]
        whole, tall = ((uvg, ur), (uvg, ur), (mg, mr), (upg, pr))[w]
        cols = pl.ds(w * da, da) if w < 2 else slice(None) if w < 3 else pl.ds(0, size)
        if which is None:
            return whole.at[half(tall, source), cols]
        return whole.at[half(tall // 2 // n, n * (2 * source + which) + k), cols]

    def z_piece(w, role, dest, k):
        return remote(
            take(w, role, y, k), put(w, role, z, y, k), z_send.at[lane(w, k) - 3, dest],
            z_recv.at[lane(w, k), z], (y, dest, t),
        )

    def z_start(w, role, dest, ks=None):
        for k in range(parts[w]) if ks is None else ks:
            z_piece(w, role, dest, k).start()

    def y_piece(w, role, source, k):
        ref = put(w, role, source, y, k)
        return remote(ref, ref, y_send.at[lane(w, k), source], y_recv.at[lane(w, k), source], to_y)

    def y_arrived(w, role, source, k):
        ref = put(w, role, source, 1 - y, k)
        remote(
            ref, ref, y_send.at[lane(w, k), source], y_recv.at[lane(w, k), source], to_y
        ).wait_recv()

    def y_all(w, role):
        for o in others:
            for k in range(parts[w]):
                y_arrived(w, role, o, k)

    def relay(w, role, source, k):
        ref = put(w, role, source, y, k)
        remote(
            ref, ref, z_send.at[lane(w, k) - 3, source], z_recv.at[lane(w, k), source], (y, source, t)
        ).wait_recv()
        y_piece(w, role, source, k).start()

    def relays(w, role, source, ks=None):
        for k in range(parts[w]) if ks is None else ks:
            relay(w, role, source, k)

    def hop(w, source, way, own=False):
        ref = put(w, 0, source, y)
        return remote(
            take(w, 0, y) if own else ref, ref, h_send.at[w, source, way],
            z_recv.at[lane(w, 0), source], (y, z + 1 - 2 * way, t),
        )

    last = z_count - 1
    goes_on = (z < last, z > 0)

    def chain(w, distance):
        for way in range(2):
            source = z - distance if way == 0 else z + distance

            @pl.when(source >= 0 if way == 0 else source <= last)
            def _():
                hop(w, source, way).wait_recv()

                @pl.when(goes_on[way])
                def _():
                    hop(w, source, way).start()

                y_piece(w, 0, source, 0).start()

    def chain_pair(w):
        way = 1 - q
        hop(w, pair, way).wait_recv()
        hop(w, pair, way).start()
        y_piece(w, 0, pair, 0).start()

    def chain_facing(w):
        way = q
        hop(w, facing, way).wait_recv()
        hop(w, facing, way).start()
        y_piece(w, 0, facing, 0).start()

    def own_copies(w, role):
        return [
            pltpu.make_async_copy(
                take(w, role, None), put(w, role, z, None), l_sem.at[w]
            )
        ]

    def link(a, n):
        return 6 + n if a == 2 else 3 * a + (1, 2, 5).index(n)

    def gather_copy(a, h, n):
        p, s, where = (
            (q, t, to_z), (q, t, to_x), (q, t, to_c), (1 - q, t, to_x), (1 - q, t, to_c),
            (q, t_chip, to_c), (1 - q, t_chip, to_c),
        )[n]
        ref = piece(a, h, p, s)
        return remote(ref, ref, a_send.at[link(a, n), h], a_recv.at[link(a, n), h], where)

    def gather_arrived(a, h, n):
        p, s, where = (
            (1 - q, t, to_z), (q, t_chip, to_x), (q, t_core, to_c), (1 - q, t_chip, to_x),
            (1 - q, t_core, to_c), (q, 3 - t, to_c), (1 - q, 3 - t, to_c),
        )[n]
        ref = piece(a, h, p, s)
        return remote(ref, ref, a_send.at[link(a, n), h], a_recv.at[link(a, n), h], where)

    def piece(a, h, p, s):
        if a == 0:
            return xg.at[s, pl.ds(h * step, step), :]
        return gat.at[s, h] if a == 1 else mid.at[p, s, pl.ds(h * step, step)]

    def gather_start(a, h):
        for n in (1, 2, 0)[: 3 if a == 2 else 2]:
            gather_copy(a, h, n).start()

    def gather_pair(a, h):
        gather_arrived(a, h, 0).wait_recv()
        gather_copy(a, h, 3).start()
        gather_copy(a, h, 4).start()

    def gather_rest(a, h):
        gather_arrived(a, h, 1).wait_recv()
        gather_copy(a, h, 5).start()
        if a == 2:
            gather_arrived(a, h, 3).wait_recv()
            gather_copy(a, h, 6).start()
        for n in (2, 4, 5, 6) if a == 2 else (2, 5):
            gather_arrived(a, h, n).wait_recv()

    chunks = rows // step
    inner = jnp.logical_and(z > 0, z < last)

    def hop_own(w):
        for way in range(2):
            @pl.when(goes_on[way])
            def _():
                hop(w, z, way, True).start()

    hop_own(0)
    hop_own(1)
    own_tok.wait()
    for h in range(chunks):
        gather_start(0, h)
    for fetch in fetches:
        fetch.wait()

    def scaled(pieces, gain):
        total = pieces[0].shape[0]
        sums = jnp.zeros((total, 1), f32)
        for piece in pieces:
            sums += jnp.sum(piece * piece, axis=-1, keepdims=True)
        count = sum(piece.shape[1] for piece in pieces)
        scale = lax.rsqrt(sums / count + EPS)
        at = 0
        res = []
        for piece in pieces:
            wide = piece.shape[1]
            res.append((piece * scale * gain[:, at : at + wide]).astype(bf16))
            at += wide
        return jnp.concatenate(res, axis=1)

    small = 64
    per_part = step // small
    gain_one = gain1[...].astype(f32).reshape(1, -1)
    gain_two = gain2[...].astype(f32).reshape(1, -1)

    def norm_one(h):
        def loop(i, carry):
            here = pl.ds(pl.multiple_of(h * step + i * small, small), small)
            norm[here, :] = scaled([xg[s, here, :].astype(f32) for s in range(4)], gain_one)
            return carry

        lax.fori_loop(0, per_part, loop, 0)

    blk = spat.shape[1]
    lower = lax.broadcasted_iota(jnp.int32, (blk, blk), 0) >= lax.broadcasted_iota(
        jnp.int32, (blk, blk), 1
    )
    eye = lax.broadcasted_iota(jnp.int32, (blk, blk), 0) == lax.broadcasted_iota(
        jnp.int32, (blk, blk), 1
    )
    mixers, shifts, gains = [], [], []
    for g in range(da // gw):
        mixers.append(jnp.where(lower, spat[g].astype(f32), 0.0).astype(bf16))
        column = jnp.where(eye, bias[g : g + 1, :].astype(f32), 0.0)
        shifts.append(jnp.sum(column, axis=1, keepdims=True))
        gains.append(ggain[g : g + 1, :].astype(f32))

    def mix_rows(h):
        both = jnp.dot(norm[pl.ds(h * step, step), :], uvg[...], preferred_element_type=f32)
        both = jax.nn.gelu(both)
        u_act = both[:, :da].astype(bf16).astype(f32)
        for g in range(da // gw):
            cols = slice(g * gw, (g + 1) * gw)
            v_act = both[:, da + g * gw : da + (g + 1) * gw]
            v_n = (
                v_act
                * lax.rsqrt(jnp.mean(v_act * v_act, axis=-1, keepdims=True) + EPS)
                * gains[g]
            ).astype(bf16)
            for b in range(step // blk):
                part = slice(b * blk, (b + 1) * blk)
                mixed = jnp.dot(mixers[g], v_n[part], preferred_element_type=f32) + shifts[g]
                gat[t, h, part, cols] = (u_act[part, cols] * mixed).astype(bf16)

    def middle_rows(h):
        left = jnp.concatenate([gat[k, h] for k in range(4)], axis=1)
        value = jnp.dot(left, mg[...], preferred_element_type=f32)
        value += xg[t, pl.ds(h * step, step), :].astype(f32)
        mid[q, t, pl.ds(h * step, step)] = value.astype(bf16)

    def norm_two(h):
        def loop(i, carry):
            p, r = i // per_part, pl.multiple_of(lax.rem(i, per_part) * small, small)
            here = pl.ds(pl.multiple_of(h * step + r, small), small)
            pieces = [mid[p, k, here, :].astype(f32) for k in range(4)]
            at = pl.multiple_of((p * chunks + h) * step + r, small)
            norm[pl.ds(at, small), :] = scaled(pieces, gain_two)
            return carry

        lax.fori_loop(0, 2 * per_part, loop, 0)

    def up_rows(h, role):
        size = share[role]

        def loop(i, carry):
            here = pl.ds(pl.multiple_of((i * chunks + h) * step, step), step)
            pre = jnp.dot(norm[here, :], upg[:, :size], preferred_element_type=f32)
            hid[here, :size] = jnp.square(jax.nn.relu(pre)).astype(bf16)
            return carry

        lax.fori_loop(0, 2, loop, 0)

    def part(quarter, k, p, role):
        size, side = share[role], slice(k * col, (k + 1) * col)
        return jnp.dot(
            hid[half_rows(p), :size], dng[quarter, :size, side], preferred_element_type=f32
        )

    def half_rows(p):
        return pl.ds(pl.multiple_of(p * rows, rows), rows)

    def core_copy(n, k):
        return remote(
            c_out.at[n, k], c_in.at[n, k], c_send.at[n, k], c_recv.at[n, k], to_c
        )

    wide_n, slim_n = c, 1 - c
    own_wide = x == c

    def wide_x(k):
        return remote(c_in.at[wide_n, k], x_in.at[k], s_send.at[k], s_recv.at[k], to_x)

    def wide_z(k):
        return remote(z_out.at[k], z_in.at[k], r_send.at[k], r_recv.at[k], to_z)

    def slim_z(k):
        return remote(
            c_in.at[slim_n, k, half_rows(1 - q)], z_part.at[k], p_send.at[k], p_recv.at[k], to_z
        )

    def slim_x(k):
        return remote(x_out.at[k], x_part.at[k], o_send.at[k], o_recv.at[k], to_x)

    def down(quarter, k, role):
        n = quarter // 2
        mine = lax.rem(quarter, 2) == c

        @pl.when(jnp.logical_not(mine))
        def _():
            def loop(p, carry):
                c_out[n, k, half_rows(p), :] = part(quarter, k, p, role).astype(bf16)
                return carry

            lax.fori_loop(0, 2, loop, 0)
            core_copy(n, k).start()

        @pl.when(mine)
        def _():
            def loop(p, carry):
                acc[half_rows(p), :] = part(quarter, k, p, role)
                return carry

            lax.fori_loop(0, 2, loop, 0)
            core_copy(n, k).wait_recv()

            def add(b, carry):
                here = pl.ds(pl.multiple_of(b * small, small), small)
                value = acc[here, :] + c_in[n, k, here, :].astype(f32)
                c_in[n, k, here, :] = value.astype(bf16)
                return carry

            lax.fori_loop(0, 2 * rows // small, add, 0)

            @pl.when((n == wide_n) & jnp.logical_not(own_wide))
            def _():
                wide_x(k).start()

            @pl.when(n == slim_n)
            def _():
                slim_z(k).start()

    sides = range(cols)
    low, high = sides[: cols // 2], sides[cols // 2 :]

    def in_rows(run):
        def loop(b, carry):
            run(
                pl.ds(pl.multiple_of(b * small, small), small),
                pl.ds(pl.multiple_of((1 - q) * rows + b * small, small), small),
                pl.ds(pl.multiple_of(q * rows + b * small, small), small),
            )
            return carry

        lax.fori_loop(0, rows // small, loop, 0)

    def meet(ks, fits=True):
        @pl.when(own_wide & fits)
        def _():
            for k in ks:
                wide_x(k).wait_recv()

                def run(here, theirs, ours):
                    value = c_in[wide_n, k, theirs, :].astype(f32)
                    value += x_in[k, theirs, :].astype(f32)
                    z_out[k, here, :] = value.astype(bf16)

                in_rows(run)
                wide_z(k).start()

    every = range(cuts)

    def mixer():
        for w in range(2):
            for copy in own_copies(w, 0):
                copy.wait()
            y_all(w, 0)
        for h in range(chunks):
            mix_rows(h)
            gather_start(1, h)

    def middle():
        for copy in own_copies(2, 0):
            copy.wait()
        y_all(2, 0)
        for h in range(chunks):
            gather_rest(1, h)
            middle_rows(h)
            gather_start(2, h)

    def up_ready(role):
        for copy in own_copies(3, role):
            copy.wait()
        y_all(3, role)
        for copy in own_copies(4, role):
            copy.wait()

    def downs(role, source, ks=None):
        per = cuts // cols
        for k in sides if ks is None else ks:
            for i in range(per):
                y_arrived(4, role, source, k * per + i)
            down(source, k, role)

    def last_downs(role, k):
        per = cuts // cols
        for source in (pair, across):
            for i in range(per):
                y_arrived(4, role, source, k * per + i)
        pair_first = lax.rem(pair, 2) != c
        down(jnp.where(pair_first, pair, across), k, role)
        down(jnp.where(pair_first, across, pair), k, role)

    def start(role):
        for w in range(5):
            for copy in own_copies(w, role):
                copy.start()

    @pl.when(jnp.logical_not(inner))
    def _():
        hop_own(2)
        start(0)
        z_start(3, 1, pair)
        z_start(3, 1, across)
        for w in range(2):
            chain(w, 1)
        for h in range(chunks):
            gather_rest(0, h)
            norm_one(h)
        for w in range(2):
            chain(w, 2)
        chain(2, 1)
        for w in range(2):
            chain(w, 3)
        chain(2, 2)
        chain(2, 3)
        mixer()
        middle()
        z_start(4, 1, across, every[:1])
        z_start(3, 0, facing)
        z_start(4, 1, pair)
        z_start(4, 0, facing)
        z_start(4, 1, across, every[1:])
        relays(3, 0, pair)
        gather_pair(2, 0)
        gather_pair(2, 1)
        gather_rest(2, 0)
        norm_two(0)
        relay(3, 0, facing, 0)
        gather_rest(2, 1)
        norm_two(1)
        relay(3, 0, facing, 1)
        relays(3, 0, across)
        relay(4, 0, across, 0)
        relay(4, 0, across, 1)
        up_ready(0)
        relay(4, 0, facing, 0)
        relay(4, 0, facing, 1)
        up_rows(0, 0)
        relay(4, 0, facing, 2)
        relay(4, 0, facing, 3)
        up_rows(1, 0)
        relay(4, 0, pair, 0)
        for k in low:
            down(z, k, 0)
        relay(4, 0, pair, 1)
        for k in high:
            down(z, k, 0)
        downs(0, across, low)
        relay(4, 0, pair, 2)
        downs(0, facing)
        relay(4, 0, across, 2)
        relay(4, 0, across, 3)
        relay(4, 0, pair, 3)
        downs(0, pair, low)
        meet(low)
        for k in high:
            last_downs(0, k)
        meet(high)

    @pl.when(inner)
    def _():
        start(1)
        for w in range(2):
            chain_pair(w)
            chain_facing(w)
        hop_own(2)
        chain_pair(2)
        z_start(3, 1, facing)
        z_start(4, 1, facing, every[:1])
        z_start(3, 0, across)
        z_start(4, 0, across)
        z_start(4, 1, facing, every[1:])
        for w in range(2):
            chain(w, 2)
        chain_facing(2)
        for h in range(chunks):
            gather_rest(0, h)
            norm_one(h)
        chain(2, 2)
        z_start(3, 0, pair)
        relays(3, 1, pair)
        mixer()
        relay(3, 1, across, 0)
        middle()
        z_start(4, 0, pair)
        relay(3, 1, across, 1)
        relay(3, 1, facing, 0)
        relay(3, 1, facing, 1)
        gather_pair(2, 0)
        gather_pair(2, 1)
        relay(4, 1, facing, 0)
        relay(4, 1, across, 0)
        gather_rest(2, 0)
        norm_two(0)
        gather_rest(2, 1)
        norm_two(1)
        relay(4, 1, pair, 0)
        up_ready(1)
        relay(4, 1, pair, 1)
        up_rows(0, 1)
        relay(4, 1, pair, 2)
        up_rows(1, 1)
        relay(4, 1, pair, 3)
        for k in low:
            down(z, k, 1)
        for k in high:
            down(z, k, 1)
        downs(1, pair)
        relay(4, 1, across, 1)
        relay(4, 1, across, 2)
        relay(4, 1, across, 3)
        downs(1, across, low)
        relay(4, 1, facing, 1)
        downs(1, across, high)
        relays(4, 1, facing, every[2:])
        meet(sides, t == pair)
        downs(1, facing)
        meet(sides, t == across)

    def result(value, k, here):
        side = slice(k * col, (k + 1) * col)
        out[here, side] = (value + residual(here, side)).astype(bf16)

    def residual(here, side):
        return mid[q, t, here, side].astype(f32)

    @pl.when(own_wide)
    def _():
        for k in sides:
            slim_z(k).wait_recv()

            def run(here, theirs, ours):
                value = c_in[slim_n, k, ours, :].astype(f32) + z_part[k, here, :].astype(f32)
                x_out[k, here, :] = value.astype(bf16)

            in_rows(run)
            slim_x(k).start()
        for k in sides:
            wide_z(k).wait_recv()

            def run(here, theirs, ours):
                value = c_in[wide_n, k, ours, :].astype(f32) + x_in[k, ours, :].astype(f32)
                result(value + z_in[k, here, :].astype(f32), k, here)

            in_rows(run)
        for k in sides:
            wide_z(k).wait_send()
            slim_x(k).wait_send()

    @pl.when(jnp.logical_not(own_wide))
    def _():
        for k in sides:
            slim_z(k).wait_recv()
            slim_x(k).wait_recv()

            def run(here, theirs, ours):
                value = c_in[slim_n, k, ours, :].astype(f32) + z_part[k, here, :].astype(f32)
                result(value + x_part[k, here, :].astype(f32), k, here)

            in_rows(run)
        for k in sides:
            wide_x(k).wait_send()

    def drain(role):
        for w in range(5):
            for o, other in ((across, 1 - role), (facing, role), (pair, 1 - role)):
                for k in range(parts[w]):
                    if w > 2:
                        z_piece(w, other, o, k).wait_send()
                    y_piece(w, role, o, k).wait_send()

    @pl.when(jnp.logical_not(inner))
    def _():
        drain(0)

    @pl.when(inner)
    def _():
        drain(1)

    for w in range(3):
        for source in range(z_count):
            for way in range(2):
                came = source <= z if way == 0 else source >= z

                @pl.when(came & goes_on[way])
                def _():
                    hop(w, source, way).wait_send()

    for h in range(chunks):
        for a in range(3):
            for n in range(7) if a == 2 else (1, 2, 5):
                gather_copy(a, h, n).wait_send()
    for k in sides:
        for n in range(2):
            core_copy(n, k).wait_send()
        slim_z(k).wait_send()


def fused(tokens, first_gain, u_proj, v_proj, group_gain, spatial, spatial_bias, mix_proj,
          second_gain, up_proj, down_proj):
    rows, width = tokens.shape
    both, wide, da = 2 * rows, second_gain.shape[0], u_proj.shape[1]
    vmem, bf16, dma = pltpu.VMEM, jnp.bfloat16, pltpu.SemaphoreType.DMA
    spec, far = (pl.BlockSpec(memory_space=m) for m in (pltpu.VMEM, pl.ANY))
    ff = up_proj.shape[1] // 16 * 9
    small = (first_gain, group_gain, spatial, spatial_bias, second_gain)
    step = 256
    chunks = rows // step
    cuts = 4
    cols = 4
    col = width // cols
    return pl.pallas_call(
        functools.partial(fused_kernel, step, cuts),
        out_shape=jax.ShapeDtypeStruct(tokens.shape, tokens.dtype),
        in_specs=[far] * 11,
        out_specs=spec,
        scratch_shapes=[
            *(vmem(v.shape, v.dtype) for v in small),
            vmem((4, rows, width), bf16),
            vmem((wide, 2 * da), bf16),
            vmem((4 * mix_proj.shape[0], width), bf16),
            vmem((wide, ff), bf16),
            vmem((4, ff, width), bf16),
            vmem((both, wide), bf16),
            vmem((4, chunks, step, da), bf16),
            vmem((2, 4, rows, width), bf16),
            vmem((both, ff), bf16),
            vmem((2, cols, both, col), bf16),
            vmem((2, cols, both, col), bf16),
            vmem((cols, rows, col), bf16),
            vmem((cols, rows, col), bf16),
            vmem((cols, rows, col), bf16),
            vmem((cols, both, col), bf16),
            vmem((cols, rows, col), bf16),
            vmem((cols, rows, col), bf16),
            vmem((both, col), jnp.float32),
            dma((3, 4, 2)),
            dma((2 + cuts, 4)), dma((5 + cuts, 4)), dma((5 + cuts, 4)), dma((5 + cuts, 4)),
            dma((11,)),
            dma((13, chunks)), dma((13, chunks)),
            dma((2, cols)), dma((2, cols)), dma((cols,)), dma((cols,)), dma((cols,)),
            dma((cols,)), dma((cols,)), dma((cols,)), dma((cols,)), dma((cols,)),
        ],
        compiler_params=pltpu.CompilerParams(
            collective_id=0, has_side_effects=True, vmem_limit_bytes=64 * 1024 * 1000
        ),
    )(
        tokens, first_gain, u_proj, v_proj, group_gain, spatial, spatial_bias, mix_proj,
        second_gain, up_proj, down_proj,
    )


def layer_part(axes, *args):
    tokens, group_gain, spatial = args[0], args[4], args[5]
    fits = (
        axes["grp"] == 2
        and axes["fs"] == 4
        and axes["tp"] == 4
        and group_gain.shape[0] == 2
        and group_gain.shape[1] % 128 == 0
        and tokens.shape[0] % 256 == 0
        and tokens.shape[1] % 256 == 0
        and tokens.shape[1] == args[10].shape[1]
        and 256 % spatial.shape[1] == 0
        and args[9].shape[1] % 2048 == 0
    )
    return fused(*args) if fits else per_device(*args)


def solution(mesh):
    return jax.shard_map(
        functools.partial(layer_part, dict(mesh.shape)),
        mesh=mesh,
        in_specs=(
            P(("grp", "fs"), "tp"),
            P(),
            P("fs", "tp"),
            P("fs", "tp"),
            P("tp", None),
            P("tp", None, None),
            P("tp", None),
            P("fs", "tp"),
            P(),
            P("fs", "tp"),
            P("tp", "fs"),
        ),
        out_specs=P(("grp", "fs"), "tp"),
        check_vma=False,
    )
```
